512 devices in a mesh: ep: 32 (over z, core), tp: 16 (over y, x).
Axes of the slice: x: 4, y: 4, z: 16, core: 2. Of those that a mesh axis runs over, the one named last changes fastest.
Arguments:
- probe_preactivations: bfloat16 [16384, 2048], P('ep', 'tp'), may hold values from -6 to 6
- rightward_retain_scores: bfloat16 [16384, 2048], P('ep', 'tp'), may hold values from -5.5 to 5.5
- leftward_retain_scores: bfloat16 [16384, 2048], P('ep', 'tp'), may hold values from -5.5 to 5.5
- payload_vectors: bfloat16 [16384, 2048], P('ep', 'tp'), may hold values from -6 to 6
- retain_minimum_bounds: float32 [2, 2048], P(None, 'tp'), may hold values from 0.88 to 1
- extra_shrink_spikes: float32 [16, 16384], P('tp', 'ep'), may hold values from -0.7 to 0
- mixer_rescale_factor: float32 [2048], P('tp'), may hold values from 0.1 to 1.9
- mixer_emit_matrix: bfloat16 [2048, 2048], P('tp'), may hold values from -0.1875 to 0.1875
- specialist_arriving_tokens: bfloat16 [4096, 2048], P('ep'), may hold values from -6 to 6
- specialist_rescale_factor: float32 [2048], replicated, may hold values from 0.1 to 1.9
- routed_specialist_ids: int32 [4096, 2], P('ep'), may hold values from 0 to 31, all different within a row; in each aligned block of 128 rows (0 to 127, 128 to 255, ...) at most 16 rows name the same one
- routed_specialist_shares: float32 [4096, 2], P('ep'), may hold values from 0.1 to 1
- specialist_switch_matrix: bfloat16 [32, 2048, 3584], P('ep', None, 'tp'), may hold values from -0.125 to 0.125
- specialist_widen_matrix: bfloat16 [32, 2048, 3584], P('ep', None, 'tp'), may hold values from -0.125 to 0.125
- specialist_shrink_matrix: bfloat16 [32, 3584, 2048], P('ep', 'tp'), may hold values from -0.125 to 0.125
Outputs:
- mixed_a: bfloat16 [16384, 2048], P('ep', 'tp')
- mixed_b: bfloat16 [4096, 2048], P('ep', 'tp')
The draws below stay inside these ranges and needn't reach their ends.
Inputs may be any that keep to these rules, and one draw needn't show every extreme that they name: `routed_specialist_ids`: each row names 2 different experts; within the rows of one index of ep no expert is named by more than 16 rows, and in every draw some expert is named by exactly 16 rows of some index.
All inputs are finite; a program needn't handle non-finite values.
Results may differ from the reference program's by a relative error of at most 0.015.
Values may be sent and summed in bfloat16 or wider, within the bound.
A program may use at most 64 MiB of HBM per device.

```python
import math
import jax
import jax.numpy as jnp
import numpy as np
from jax import lax

D = 2048
MIXER_STREAMS = 16
DK = 128
DE = 3584
TOP_K = 2
SPAN = 32
TOK_A = 512
TOK_B = 128
DV = 128
F = 2048
SEQ = 16384
ROWS_B = 4096
EXPERTS = 32
CAP = 16
N_EP = 32
N_TP = 16


def forget_draw(key):
    noise_key, offset_key = jax.random.split(key)
    noise = jnp.clip(jax.random.normal(noise_key, (SEQ, F), jnp.float32), -4.0, 4.0)
    offsets = jax.random.uniform(offset_key, (SEQ // TOK_A, 1, F), jnp.float32, -1.5, 1.5)
    shifted = noise.reshape(SEQ // TOK_A, TOK_A, F) + offsets
    return shifted.reshape(SEQ, F).astype(jnp.bfloat16)


def draw_rightward_retain_scores(key, part):
    return forget_draw(jax.random.fold_in(key, 11))


def draw_leftward_retain_scores(key, part):
    return forget_draw(jax.random.fold_in(key, 12))


def draw_retain_minimum_bounds(key, part):
    kind_key, slow_key, fast_key = jax.random.split(jax.random.fold_in(key, 21), 3)
    slow_head = jax.random.randint(kind_key, (2, MIXER_STREAMS, 1), 0, 2) > 0
    slow_gap = jax.random.uniform(slow_key, (2, MIXER_STREAMS, DK), jnp.float32, 0.5, 2.0) / SEQ
    fast_gap = jnp.exp(jax.random.uniform(fast_key, (2, MIXER_STREAMS, DK), jnp.float32, -3.2, -2.13))
    chosen_gap = jnp.where(slow_head, slow_gap, fast_gap)
    return (1.0 - chosen_gap).reshape(2, F).astype(jnp.float32)


def draw_extra_shrink_spikes(key, part):
    where_key, depth_key = jax.random.split(jax.random.fold_in(key, 31))
    struck = jax.random.randint(where_key, (MIXER_STREAMS, SEQ), 0, SEQ) < 6
    depth = jnp.log(1.0 - jax.random.uniform(depth_key, (MIXER_STREAMS, SEQ), jnp.float32, 0.2, 0.5))
    return jnp.where(struck, depth, 0.0).astype(jnp.float32)


def strengthened(entries, key, source, target, shards_of, factor):
    def block_of(dim):
        return (jnp.arange(entries.shape[dim]) // (entries.shape[dim] // shards_of)).reshape((-1,) + (1,) * (entries.ndim - 1 - dim))

    first = jax.random.permutation(key, shards_of)[block_of(target)]
    second = (block_of(target) + shards_of // 2) % shards_of
    return jnp.where((block_of(source) == first) | (block_of(source) == second), factor * entries, entries)


def steps_of(own_key, dims, cuts, smallest, top_value):
    def one(axis_at, blocks):
        draws = jax.random.uniform(jax.random.fold_in(jax.random.fold_in(own_key, 6), axis_at), (blocks,), jnp.float32, smallest / len(cuts), top_value / len(cuts))
        return jnp.repeat(jnp.exp(draws), dims[axis_at] // blocks).reshape((-1,) + (1,) * (len(dims) - axis_at - 1))

    gain = one(*cuts[0])
    for cut in cuts[1:]:
        gain = gain * one(*cut)
    return gain


def deal_out(rng, own, number, rows, number_of, top, limit, skew):
    order = jax.random.permutation(rng, number_of)
    packed, usual = shares(number_of, rows * top, limit, skew, True), shares(number_of, rows * top, limit, skew, False)
    places = jnp.arange(number_of)

    def named(sizes, rotation):
        used = int((sizes > 0).sum())
        fixed = max(1, used // 4)
        moved = fixed + (places - fixed + rotation * (used - fixed)) % max(1, number_of - fixed)
        return jnp.zeros((number_of,), jnp.int32).at[order[jnp.where(places < fixed, places, moved)]].set(jnp.asarray(sizes, jnp.int32))

    sizes = jnp.where(number % 4 == 0, named(packed, number // 4), named(usual, number - number // 4 - 1))
    mixed = jax.random.permutation(jax.random.fold_in(own, 3), number_of)
    giver, sink = mixed[0:number_of // 2 * 2:2], mixed[1:number_of // 2 * 2:2]
    slack = jnp.minimum(sizes[giver] - 1, limit - sizes[sink]) // 2
    slack = jnp.where((giver == order[0]) | (sink == order[0]) | (sizes[sink] == 0), 0, jnp.maximum(slack, 0))
    moved = jax.random.randint(jax.random.fold_in(own, 4), (number_of // 2,), 0, 1 << 20) % (slack + 1)
    sizes = sizes.at[giver].add(-moved).at[sink].add(moved)
    items = jnp.searchsorted(jnp.cumsum(sizes), jnp.arange(rows * top), side="right").astype(jnp.int32)
    table = items.reshape(top, rows).T
    table = table[jax.random.permutation(jax.random.fold_in(own, 1), rows)]
    rotation = jax.random.randint(jax.random.fold_in(own, 2), (rows, 1), 0, top)
    return jnp.take_along_axis(table, (jnp.arange(top)[None, :] + rotation) % top, axis=1)


def shares(number_of, total, most, lean, full):
    weights = [(1 << 20) // math.isqrt(standing ** lean) + 1 for standing in range(1, number_of + 1)]
    largest = most if full else min(most, max(-(-total // number_of), total * weights[0] // sum(weights)))
    least = 1 if total - largest >= number_of - 1 else 0
    holding, rest = [largest] + [least] * (number_of - 1), total - largest - least * (number_of - 1)
    while rest > 0:
        candidates = [i for i in range(1, number_of) if holding[i] < largest] or [i for i in range(1, number_of) if holding[i] < most]
        mass, left = sum([weights[i] for i in candidates]), rest
        for i in candidates:
            more = min(most - holding[i], max(1, left * weights[i] // mass), rest)
            holding[i] = holding[i] + more
            rest = rest - more
    return np.array(holding)


def gaussian(own_key, dims, deviation, most, cuts=(), kind=jnp.bfloat16):
    entries = jax.random.normal(own_key, dims, jnp.float32) * deviation
    if len(cuts) > 0:
        entries = steps_of(own_key, dims, cuts, -0.22, 0.18) * entries
    return jnp.clip(entries, min=-most, max=most).astype(kind)


def gaussian_with(key, shape, deviation, most, cuts, heavy, kind=jnp.bfloat16):
    result = deviation * jax.random.normal(key, shape, jnp.float32)
    if cuts:
        result = result * steps_of(key, shape, cuts, -0.22, 0.18)
    return jnp.clip(strengthened(result, jax.random.fold_in(key, 3), *heavy), -most, most).astype(kind)


def setup_inputs(seed: int = 0) -> dict:
    keys = jax.random.split(jax.random.key(seed), 16)
    probe_preactivations = gaussian(keys[0], (SEQ, F), 1.0, 6.0, ((0, 32), (1, 16)))
    rightward_retain_scores = draw_rightward_retain_scores(jax.random.fold_in(keys[15], 71), 0)
    leftward_retain_scores = draw_leftward_retain_scores(jax.random.fold_in(keys[15], 71), 0)
    payload_vectors = gaussian(keys[3], (SEQ, D), 1.0, 6.0, ((0, 32), (1, 16)))
    retain_minimum_bounds = draw_retain_minimum_bounds(jax.random.fold_in(keys[15], 71), 0)
    extra_shrink_spikes = draw_extra_shrink_spikes(jax.random.fold_in(keys[15], 71), 0)
    mixer_rescale_factor = jnp.clip(1.0 + 0.18 * jax.random.normal(keys[6], (D,), jnp.float32), 0.1, 1.9)
    mixer_emit_matrix = gaussian_with(keys[7], (D, D), D ** -0.5, 0.1875, ((0, 16),), (0, 1, 16, 2.0))
    specialist_arriving_tokens = gaussian(keys[8], (ROWS_B, D), 1.0, 6.0, ((0, 32),))
    specialist_rescale_factor = jnp.clip(1.0 + 0.18 * jax.random.normal(keys[9], (D,), jnp.float32), 0.1, 1.9)
    routed_specialist_ids_keys = jax.random.split(jax.random.fold_in(keys[10], 1), ROWS_B // TOK_B)
    routed_specialist_ids_turns = jax.random.permutation(jax.random.fold_in(keys[10], 3), ROWS_B // TOK_B)
    routed_specialist_ids = jax.vmap(lambda own, number: deal_out(jax.random.fold_in(keys[10], 2), own, number, TOK_B, EXPERTS, TOP_K, CAP, 2))(routed_specialist_ids_keys, routed_specialist_ids_turns).reshape((ROWS_B, TOP_K))
    routed_specialist_shares = jnp.clip(0.1 + 0.9 * jax.random.uniform(keys[11], (ROWS_B, TOP_K), jnp.float32) ** steps_of(keys[11], (ROWS_B, TOP_K), ((0, 32),), -0.2, 0.2), 0.1, 1.0)
    specialist_switch_matrix = gaussian(keys[12], (EXPERTS, D, DE), D ** -0.5, 0.125, ((0, 32), (2, 16)))
    specialist_widen_matrix = gaussian(keys[13], (EXPERTS, D, DE), D ** -0.5, 0.125, ((0, 32), (2, 16)))
    specialist_shrink_matrix = gaussian_with(keys[14], (EXPERTS, DE, D), DE ** -0.5, 0.125, ((0, 32), (1, 16)), (1, 2, 16, 2.0))
    return {"probe_preactivations": probe_preactivations, "rightward_retain_scores": rightward_retain_scores, "leftward_retain_scores": leftward_retain_scores, "payload_vectors": payload_vectors, "retain_minimum_bounds": retain_minimum_bounds, "extra_shrink_spikes": extra_shrink_spikes, "mixer_rescale_factor": mixer_rescale_factor, "mixer_emit_matrix": mixer_emit_matrix, "specialist_arriving_tokens": specialist_arriving_tokens, "specialist_rescale_factor": specialist_rescale_factor, "routed_specialist_ids": routed_specialist_ids, "routed_specialist_shares": routed_specialist_shares, "specialist_switch_matrix": specialist_switch_matrix, "specialist_widen_matrix": specialist_widen_matrix, "specialist_shrink_matrix": specialist_shrink_matrix}


EPS = 1e-06
NEG_BIG = -1e+30
HIGH_PRECISION = lax.Precision.HIGHEST

def recurrence(query_heads, key_gate, v_heads, shrink_exponent, state_in):
    channel_group_count, length, _ = query_heads.shape
    block_count = length // SPAN

    def blocks(tensor):
        return jnp.moveaxis(tensor.reshape(channel_group_count, block_count, SPAN, tensor.shape[-1]), 1, 0)
    lower_tri = jnp.tril(jnp.ones((SPAN, SPAN), dtype=bool))[:, :, None]

    def advance(carried_state, pieces):
        query_block, key_block, value_block, l_blk = pieces
        cumulative_decay = jnp.cumsum(l_blk, axis=1)
        block_final_state = cumulative_decay[:, -1:, :]
        relative = cumulative_decay[:, :, None, :] - cumulative_decay[:, None, :, :]
        decays = jnp.exp(jnp.where(lower_tri, relative, NEG_BIG))
        scores = jnp.einsum('htk,hsk,htsk->hts', query_block, key_block, decays, precision=HIGH_PRECISION)
        block_result = jnp.einsum('hts,hsv->htv', scores, value_block, precision=HIGH_PRECISION)
        block_result = block_result + jnp.einsum('dyr,dru->dyu', query_block * jnp.exp(cumulative_decay), carried_state, precision=HIGH_PRECISION)
        carried_state = jnp.exp(block_final_state[:, 0, :])[:, :, None] * carried_state + jnp.einsum('qfw,qfa->qwa', key_block * jnp.exp(block_final_state - cumulative_decay), value_block, precision=HIGH_PRECISION)
        return (carried_state, block_result)
    final_state, block_outs = lax.scan(advance, state_in, (blocks(query_heads), blocks(key_gate), blocks(v_heads), blocks(shrink_exponent)))
    return (jnp.moveaxis(block_outs, 0, 1).reshape(channel_group_count, length, v_heads.shape[-1]), final_state)

def to_heads(matrix, channel_group_count):
    length = matrix.shape[0]
    return matrix.astype(jnp.float32).reshape(length, channel_group_count, -1).transpose(1, 0, 2)

def retain_factors(retain_scores, retain_minimum, extra_shrink_spikes, channel_group_count):
    pre_act = to_heads(retain_scores, channel_group_count)
    floor_b = retain_minimum.reshape(channel_group_count, 1, -1)
    retain_factor = floor_b + (1.0 - floor_b) * jax.nn.sigmoid(pre_act)
    shrink_exponent = jnp.log(retain_factor) + extra_shrink_spikes[:, :, None]
    key_gate = (1.0 - floor_b) * jax.nn.sigmoid(-pre_act)
    return (key_gate, shrink_exponent)

def reverse_seq(tensor):
    return jnp.flip(tensor, axis=1)

def rounded(partial_value):
    return lax.optimization_barrier(partial_value.astype(jnp.bfloat16)).astype(jnp.float32)

def reference(probe_preactivations, rightward_retain_scores, leftward_retain_scores, payload_vectors, retain_minimum_bounds, extra_shrink_spikes, mixer_rescale_factor, mixer_emit_matrix, specialist_arriving_tokens, specialist_rescale_factor, routed_specialist_ids, routed_specialist_shares, specialist_switch_matrix, specialist_widen_matrix, specialist_shrink_matrix):
    query_heads = jax.nn.silu(to_heads(probe_preactivations, MIXER_STREAMS))
    v_heads = to_heads(payload_vectors, MIXER_STREAMS)
    rightward_seed, rightward_shrink_exponent = retain_factors(rightward_retain_scores, retain_minimum_bounds[0], extra_shrink_spikes, MIXER_STREAMS)
    leftward_seed, leftward_shrink_exponent = retain_factors(leftward_retain_scores, retain_minimum_bounds[1], extra_shrink_spikes, MIXER_STREAMS)
    zero_state = jnp.zeros((MIXER_STREAMS, DK, DV), jnp.float32)
    out_fwd, _ = recurrence(query_heads, rightward_seed, v_heads, rightward_shrink_exponent, zero_state)
    out_bwd, _ = recurrence(reverse_seq(query_heads), reverse_seq(leftward_seed), reverse_seq(v_heads), reverse_seq(leftward_shrink_exponent), zero_state)
    combined = out_fwd + reverse_seq(out_bwd)
    normed = combined * lax.rsqrt(lax.optimization_barrier(jnp.mean(combined * combined, axis=-1, keepdims=True)) + EPS)
    normed = normed * mixer_rescale_factor.reshape(MIXER_STREAMS, 1, DV)
    mixed_heads = normed.transpose(1, 0, 2).reshape(SEQ, D).astype(jnp.bfloat16)
    head_groups = mixed_heads.reshape(SEQ, N_TP, D // N_TP).transpose(1, 0, 2)
    weight_groups = mixer_emit_matrix.reshape(N_TP, D // N_TP, D)

    def add_group(running, operands):
        partial_value = jnp.dot(operands[0], operands[1], preferred_element_type=jnp.float32)
        return (running + rounded(partial_value), None)
    summed_a, _ = lax.scan(add_group, jnp.zeros((SEQ, D), jnp.float32), (head_groups, weight_groups))
    mixed_a = summed_a.astype(jnp.bfloat16)
    rows_f = specialist_arriving_tokens.astype(jnp.float32)
    normed_b = (rows_f * lax.rsqrt(lax.optimization_barrier(jnp.mean(rows_f * rows_f, axis=-1, keepdims=True)) + EPS) * specialist_rescale_factor).astype(jnp.bfloat16)
    flat_ids = routed_specialist_ids.reshape(-1).astype(jnp.int32)
    onehot = (flat_ids[:, None] == jnp.arange(EXPERTS, dtype=jnp.int32)[None, :]).astype(jnp.int32)
    ranking = lax.optimization_barrier(jnp.sum((jnp.cumsum(onehot, axis=0) - onehot) * onehot, axis=1)).astype(jnp.int32)
    slot_total = N_EP * CAP
    position = (flat_ids * slot_total + ranking).astype(jnp.int32)
    copy_row = (jnp.arange(flat_ids.shape[0], dtype=jnp.int32) // TOP_K).astype(jnp.int32)
    row_table = jnp.zeros((EXPERTS * slot_total,), jnp.int32).at[position].set(copy_row).reshape(EXPERTS, slot_total)
    live_table = jnp.zeros((EXPERTS * slot_total,), jnp.bfloat16).at[position].set(1.0).reshape(EXPERTS, slot_total)

    def run_expert(operands):
        gate_w, up_w, down_w, row_index, live_slot = operands
        gathered = normed_b[row_index] * live_slot[:, None]
        gate_out = jnp.dot(gathered, gate_w, preferred_element_type=jnp.float32)
        up_out = jnp.dot(gathered, up_w, preferred_element_type=jnp.float32)
        hidden = (jax.nn.silu(gate_out) * up_out).astype(jnp.bfloat16)
        hidden_groups = hidden.reshape(slot_total, N_TP, DE // N_TP).transpose(1, 0, 2)
        down_groups = down_w.reshape(N_TP, DE // N_TP, D)
        summed, _ = lax.scan(add_group, jnp.zeros((slot_total, D), jnp.float32), (hidden_groups, down_groups))
        return summed.astype(jnp.bfloat16)
    expert_out = lax.map(run_expert, (specialist_switch_matrix, specialist_widen_matrix, specialist_shrink_matrix, row_table, live_table))
    picked = expert_out.reshape(EXPERTS * slot_total, D)[position].astype(jnp.float32)
    picked = picked.reshape(ROWS_B, TOP_K, D)
    mixed_b = lax.optimization_barrier(jnp.sum(picked * routed_specialist_shares[:, :, None], axis=1)).astype(jnp.bfloat16)
    return (mixed_a, mixed_b)
```

```python
import functools

import jax
import jax.numpy as jnp
from jax import lax
from jax.experimental import pallas as pl
from jax.experimental.pallas import tpu as pltpu
from jax.sharding import Mesh
from jax.sharding import PartitionSpec as P

EPS = 1e-06
CAP = 16
LANES = 128
CHUNK = 128
MESH = pl.DeviceIdType.MESH
F32 = jnp.float32
BF16 = jnp.bfloat16


def nn(a, b):
    return lax.dot_general(a, b, (((1,), (0,)), ((), ())), preferred_element_type=F32)


def nt(a, b):
    return lax.dot_general(a, b, (((1,), (1,)), ((), ())), preferred_element_type=F32)


def tn(a, b):
    return lax.dot_general(a, b, (((0,), (0,)), ((), ())), preferred_element_type=F32)


def iota(shape, dim):
    return lax.broadcasted_iota(jnp.int32, shape, dim)


def three_parts(a):
    hi = a.astype(BF16).astype(F32)
    rest = a - hi
    mid = rest.astype(BF16).astype(F32)
    return hi, mid, (rest - mid).astype(BF16).astype(F32)


def send(src, dst, send_sem, recv_sem, device):
    copy = pltpu.make_async_remote_copy(
        src_ref=src,
        dst_ref=dst,
        send_sem=send_sem,
        recv_sem=recv_sem,
        device_id=device,
        device_id_type=MESH,
    )
    copy.start()
    return copy


class Ring:
    def __init__(self, z, c, y, x):
        self.z, self.c, self.y, self.x = z, c, y, x

    def along(self, axis, step):
        return lax.rem((self.x if axis == 0 else self.y) + step, 4)

    def device(self, axis, step):
        there = self.along(axis, step)
        return (self.z, self.c, self.y, there) if axis == 0 else (self.z, self.c, there, self.x)


class Gather:
    ORDER = (0, 3, 1, 2)

    def __init__(self, ring, buf, send_sems, recv_sems):
        self.ring, self.buf = ring, buf
        self.send_sems, self.recv_sems = send_sems, recv_sems
        self.rows = buf.shape[2]
        self.sent = []

    def block(self, half, first, second, part):
        a, b = self.ring.along(half, first), self.ring.along(1 - half, second)
        y, x = (b, a) if half == 0 else (a, b)
        n = self.rows // 2
        start, size = {None: (0, n), 0: (0, n // 2), 1: (n // 2, n // 2)}[part]
        return self.buf.at[y, x, pl.ds(half * n + start, size), :]

    def go(self, half, axis, step, block, k):
        self.sent.append(
            send(
                block,
                block,
                self.send_sems.at[half, k],
                self.recv_sems.at[half, k],
                self.ring.device(axis, step),
            )
        )

    def arrived(self, half, block, k):
        pltpu.make_async_copy(block, block, self.recv_sems.at[half, k]).wait()

    def second(self, half, n):
        first = self.ORDER[n]
        block = self.block(half, first, 0, None)
        self.go(half, 1 - half, 1, block, 4 + 4 * n)
        self.go(half, 1 - half, 3, block, 5 + 4 * n)

    def start(self):
        for half in range(2):
            block = self.block(half, 0, 0, None)
            self.go(half, half, 1, block, 0)
            self.go(half, half, 3, block, 1)
        for half in range(2):
            self.second(half, 0)

    def near(self):
        for half in range(2):
            self.arrived(half, self.block(half, 3, 0, None), 0)
            self.go(half, half, 1, self.block(half, 3, 0, 0), 2)
            self.arrived(half, self.block(half, 1, 0, None), 1)
            self.go(half, half, 3, self.block(half, 1, 0, 1), 3)
        for half in range(2):
            self.second(half, 1)
            self.second(half, 2)

    def far(self):
        for half in range(2):
            self.arrived(half, self.block(half, 2, 0, 0), 2)
            self.arrived(half, self.block(half, 2, 0, 1), 3)
            self.second(half, 3)

    def relay(self, n):
        first = self.ORDER[n]
        for half in range(2):
            self.arrived(half, self.block(half, first, 3, None), 4 + 4 * n)
            self.go(half, 1 - half, 1, self.block(half, first, 3, 0), 6 + 4 * n)
            self.arrived(half, self.block(half, first, 1, None), 5 + 4 * n)
            self.go(half, 1 - half, 3, self.block(half, first, 1, 1), 7 + 4 * n)

    def finish(self, half):
        for n in range(4):
            first = self.ORDER[n]
            self.arrived(half, self.block(half, first, 2, 0), 6 + 4 * n)
            self.arrived(half, self.block(half, first, 2, 1), 7 + 4 * n)

    def drain(self):
        for copy in self.sent:
            copy.wait_send()


class Scatter:
    ORDER = (2, 1, 3, 0)

    def __init__(self, ring, part, far, near, last_far, last_near, out, send_sems, recv_sems):
        self.ring, self.part, self.out = ring, part, out
        self.far, self.near, self.last_far, self.last_near = far, near, last_far, last_near
        self.send_sems, self.recv_sems = send_sems, recv_sems
        self.n = part.shape[2] // 2
        self.sent = []

    def block(self, half, first, second, lo, size):
        axis = 1 - half
        a, b = self.ring.along(axis, first), self.ring.along(1 - axis, second)
        y, x = (a, b) if axis == 1 else (b, a)
        return self.part.at[y, x, pl.ds(half * self.n + lo, size), :]

    def go(self, half, axis, step, src, dst, k):
        self.sent.append(
            send(
                src,
                dst,
                self.send_sems.at[half, k],
                self.recv_sems.at[half, k],
                self.ring.device(axis, step),
            )
        )

    def arrived(self, half, ref, k):
        pltpu.make_async_copy(ref, ref, self.recv_sems.at[half, k]).wait()

    def start(self, half):
        q = self.n // 2
        for m in range(4):
            o = self.ORDER[m]
            self.go(half, 1 - half, 1, self.block(half, 2, o, 0, q), self.far.at[half, 0, m], 4 * m)
            self.go(half, 1 - half, 3, self.block(half, 2, o, q, q), self.far.at[half, 1, m], 4 * m + 1)

    def pass_on(self, half, m):
        q, o = self.n // 2, self.ORDER[m]
        for way, step in ((0, 1), (1, 3)):
            come = self.far.at[half, way, m]
            self.arrived(half, come, 4 * m + way)
            mine = self.block(half, step, o, way * q, q)
            mine[...] = (mine[...].astype(F32) + come[...].astype(F32)).astype(BF16)
            self.go(
                half,
                1 - half,
                step,
                self.block(half, step, o, 0, self.n),
                self.near.at[half, way, m],
                4 * m + 2 + way,
            )

    def collect(self, half, m):
        o = self.ORDER[m]
        for way in range(2):
            self.arrived(half, self.near.at[half, way, m], 4 * m + 2 + way)
        mine = self.block(half, 0, o, 0, self.n)
        total = mine[...].astype(F32) + self.near[half, 0, m].astype(F32)
        mine[...] = (total + self.near[half, 1, m].astype(F32)).astype(BF16)
        q = self.n // 2
        if m == 0:
            self.go(half, half, 1, self.block(half, 0, 2, 0, q), self.last_far.at[half, 0], 16)
            self.go(half, half, 3, self.block(half, 0, 2, q, q), self.last_far.at[half, 1], 17)

    def last_pass(self, half):
        q = self.n // 2
        for way, step in ((0, 1), (1, 3)):
            come = self.last_far.at[half, way]
            self.arrived(half, come, 16 + way)
            mine = self.block(half, 0, step, way * q, q)
            mine[...] = (mine[...].astype(F32) + come[...].astype(F32)).astype(BF16)
            self.go(
                half,
                half,
                step,
                self.block(half, 0, step, 0, self.n),
                self.last_near.at[half, way],
                18 + way,
            )

    def end(self, half):
        for way in range(2):
            self.arrived(half, self.last_near.at[half, way], 18 + way)
        total = self.block(half, 0, 0, 0, self.n)[...].astype(F32)
        total = total + self.last_near[half, 0].astype(F32) + self.last_near[half, 1].astype(F32)
        self.out[pl.ds(half * self.n, self.n), :] = total.astype(BF16)

    def drain(self):
        for copy in self.sent:
            copy.wait_send()


def kernel(
    ep_count,
    q_ref,
    right_ref,
    left_ref,
    v_ref,
    bounds_ref,
    spikes_ref,
    gain_ref,
    emit_ref,
    rows_ref,
    rows_gain_ref,
    ids_ref,
    shares_ref,
    switch_ref,
    widen_ref,
    shrink_ref,
    out_a_ref,
    out_b_ref,
    switch_buf,
    widen_buf,
    shrink_buf,
    emit_buf,
    outgoing,
    ebuf,
    part,
    far,
    near,
    last_far,
    last_near,
    expert_out,
    returned,
    picks,
    intra,
    query_f,
    query_b,
    added_f,
    added_b,
    chunk_decay,
    leg1_out,
    leg1_in,
    leg2_out,
    leg2_in,
    mbuf,
    load_sems,
    all_send,
    all_recv,
    eg_send,
    eg_recv,
    mg_send,
    mg_recv,
    rs_send,
    rs_recv,
):
    z, c = lax.axis_index("z"), lax.axis_index("c")
    y, x = lax.axis_index("y"), lax.axis_index("x")
    s, t = 2 * z + c, 4 * y + x
    ring = Ring(z, c, y, x)
    tok = q_ref.shape[0]
    chunks = tok // CHUNK
    rows_b = rows_ref.shape[0]
    slots = ep_count * CAP

    def ep_peer(k):
        other = lax.rem(s + k, ep_count)
        return other, (lax.div(other, 2), lax.rem(other, 2), y, x)

    def tp_peer(k):
        other = lax.rem(t + k, 16)
        return other, (z, c, lax.div(other, 4), lax.rem(other, 4))

    barrier = pltpu.get_barrier_semaphore()

    def greet_ep(k, _):
        pl.semaphore_signal(barrier, inc=1, device_id=ep_peer(k)[1], device_id_type=MESH)
        return _

    def greet_tp(k, _):
        pl.semaphore_signal(barrier, inc=1, device_id=tp_peer(k)[1], device_id_type=MESH)
        return _

    lax.fori_loop(1, ep_count, greet_ep, 0)
    lax.fori_loop(1, 16, greet_tp, 0)

    loads = [
        pltpu.make_async_copy(src, dst, load_sems.at[i])
        for i, (src, dst) in enumerate(
            (
                (switch_ref.at[0], switch_buf),
                (widen_ref.at[0], widen_buf),
                (shrink_ref.at[0], shrink_buf),
                (
                    emit_ref.at[:, pl.ds(pl.multiple_of(t * LANES, LANES), LANES)],
                    emit_buf.at[pl.ds(pl.multiple_of(t * LANES, LANES), LANES), :],
                ),
            )
        )
    ]
    for load in loads:
        load.start()

    width = rows_ref.shape[1]
    square = jnp.zeros((rows_b, LANES), F32)
    for k in range(width // LANES):
        piece = rows_ref[:, k * LANES : (k + 1) * LANES].astype(F32)
        square = square + piece * piece
    mean = jnp.sum(square, axis=1, keepdims=True) / width
    own_columns = pl.ds(pl.multiple_of(t * LANES, LANES), LANES)
    normed = rows_ref[:, own_columns].astype(F32) * lax.rsqrt(mean + EPS)
    normed = (normed * rows_gain_ref[:, own_columns]).astype(BF16)
    experts = iota((ep_count, rows_b), 0)
    pick0 = ids_ref[0:1, :] == experts
    pick1 = ids_ref[1:2, :] == experts
    named = (pick0 | pick1).astype(F32).astype(BF16)
    earlier = (iota((rows_b, rows_b), 0) < iota((rows_b, rows_b), 1)).astype(F32).astype(BF16)
    rank = nn(named, earlier)
    at_slot = rank.astype(jnp.int32)[:, None, :] == iota((ep_count, CAP, rows_b), 1)
    ones = jnp.where(at_slot, 1.0, 0.0)
    for k, pick in enumerate((pick0, pick1)):
        chosen = ones * jnp.where(pick, 1.0, 0.0)[:, None, :]
        picks[k] = chosen.reshape(slots, rows_b).astype(BF16)
    outgoing[...] = nn(picks[0] + picks[1], normed).astype(BF16)
    own_slots = pl.ds(pl.multiple_of(s * CAP, CAP), CAP)
    ebuf[y, x, own_slots, :] = outgoing[own_slots, :]

    pl.semaphore_wait(barrier, ep_count - 1 + 15)

    def dispatch(k, _):
        other, device = ep_peer(k)
        send(
            outgoing.at[pl.ds(pl.multiple_of(other * CAP, CAP), CAP), :],
            ebuf.at[y, x, own_slots, :],
            all_send.at[0],
            all_recv.at[0],
            device,
        )
        return _

    lax.fori_loop(1, ep_count, dispatch, 0)

    tri = iota((CHUNK, CHUNK), 0) >= iota((CHUNK, CHUNK), 1)
    tri_t = iota((CHUNK, CHUNK), 0) <= iota((CHUNK, CHUNK), 1)
    for n in range(chunks):
        at = slice(n * CHUNK, (n + 1) * CHUNK)
        query = q_ref[at, :].astype(F32)
        query = query * jax.nn.sigmoid(query)
        values = v_ref[at, :]
        spike = spikes_ref[0:1, at]
        scores = []
        for d, (pre_ref, mask, queries, added) in enumerate(
            ((right_ref, tri, query_f, added_f), (left_ref, tri_t, query_b, added_b))
        ):
            pre = pre_ref[at, :].astype(F32)
            bound = bounds_ref[d : d + 1, :]
            gap = 1.0 - bound
            log_decay = jnp.log(bound + gap * jax.nn.sigmoid(pre))
            key = gap * jax.nn.sigmoid(-pre)
            split = jnp.concatenate(three_parts(log_decay), axis=1).astype(BF16)
            summed = nn(jnp.where(mask, 1.0, 0.0).astype(BF16), split)
            total = summed[:, :LANES] + summed[:, LANES : 2 * LANES] + summed[:, 2 * LANES :]
            total = total + jnp.sum(jnp.where(mask, spike, 0.0), axis=1, keepdims=True)
            whole = total[CHUNK - 1 : CHUNK, :] if d == 0 else total[0:1, :]
            middle = total[CHUNK // 2 : CHUNK // 2 + 1, :]
            near_q = (query * jnp.exp(total - middle)).astype(BF16)
            near_k = (key * jnp.exp(middle - total)).astype(BF16)
            scores.append(jnp.where(mask, nt(near_q, near_k), 0.0))
            queries[at, :] = (query * jnp.exp(total)).astype(BF16)
            added[n] = tn(values, (key * jnp.exp(whole - total)).astype(BF16))
            chunk_decay[d, n] = whole
        intra[at, :] = nn((scores[0] + scores[1]).astype(BF16), values)

    z_count = ep_count // 2
    rows_s = LANES // z_count
    for d, (added, order) in enumerate(
        ((added_f, range(chunks)), (added_b, range(chunks - 1, -1, -1)))
    ):
        state, decay = None, None
        for n in order:
            state = added[n] if state is None else state * jnp.exp(chunk_decay[d, n]) + added[n]
            decay = chunk_decay[d, n] if decay is None else decay + chunk_decay[d, n]
        hi, mid, lo = three_parts(decay)
        row = iota((8, LANES), 0)
        tail = jnp.where(row == 0, hi, jnp.where(row == 1, mid, jnp.where(row == 2, lo, 0.0)))
        tail = jnp.broadcast_to(tail[None], (z_count, 8, LANES))
        leg1_out[:, d] = jnp.concatenate(
            [state.reshape(z_count, rows_s, LANES), tail], axis=1
        ).astype(BF16)

    def leg1(k, _):
        other, device = ep_peer(k)
        send(
            leg1_out.at[lax.div(other, 2), lax.rem(other, 2)],
            leg1_in.at[s],
            all_send.at[1],
            all_recv.at[1],
            device,
        )
        return _

    lax.fori_loop(1, ep_count, leg1, 0)
    leg1_in[s] = leg1_out[z, c]

    own_rows = pl.ds(pl.multiple_of(t * LANES, LANES), LANES)

    def deal(k, _):
        other, device = tp_peer(k)
        send(
            emit_ref.at[:, pl.ds(pl.multiple_of(other * LANES, LANES), LANES)],
            emit_buf.at[own_rows, :],
            all_send.at[4],
            all_recv.at[4],
            device,
        )
        return _

    def all_arrived(ref, k):
        pltpu.make_async_copy(ref, ref, all_recv.at[k]).wait()

    slots_in = ebuf.at[y, x, pl.ds(0, slots - CAP), :]
    all_arrived(slots_in, 0)
    gather_e = Gather(ring, ebuf, eg_send, eg_recv)
    gather_e.start()
    gather_e.near()

    all_arrived(leg1_in.at[pl.ds(0, ep_count - 1)], 1)
    carried = jnp.zeros((rows_s, LANES), F32)
    for n in range(ep_count):
        i = jnp.where(c == 0, n, ep_count - 1 - n)
        tile = leg1_in[i].astype(F32)
        leg2_out[i] = carried.astype(BF16)
        decay = tile[rows_s : rows_s + 1] + tile[rows_s + 1 : rows_s + 2] + tile[rows_s + 2 : rows_s + 3]
        carried = carried * jnp.exp(decay) + tile[:rows_s]

    def leg2(k, _):
        other, device = ep_peer(k)
        send(leg2_out.at[other], leg2_in.at[s], all_send.at[2], all_recv.at[2], device)
        return _

    lax.fori_loop(1, ep_count, leg2, 0)
    leg2_in[s] = leg2_out[s]

    gather_e.far()
    lax.fori_loop(1, 16, deal, 0)
    for n in range(3):
        gather_e.relay(n)

    all_arrived(leg2_in.at[pl.ds(0, ep_count - 1)], 2)
    entries = [
        jnp.concatenate([leg2_in[2 * k + d].astype(F32) for k in range(z_count)], axis=0)
        for d in range(2)
    ]
    for d, (added, queries, order) in enumerate(
        ((added_f, query_f, range(chunks)), (added_b, query_b, range(chunks - 1, -1, -1)))
    ):
        state = entries[d]
        for n in order:
            at = slice(n * CHUNK, (n + 1) * CHUNK)
            intra[at, :] += nt(queries[at, :], state.astype(BF16))
            state = state * jnp.exp(chunk_decay[d, n]) + added[n]
    mixed = intra[...]
    mixed = mixed * lax.rsqrt(jnp.mean(mixed * mixed, axis=1, keepdims=True) + EPS)
    mbuf[y, x] = (mixed * gain_ref[...]).astype(BF16)
    gather_e.relay(3)
    gather_m = Gather(ring, mbuf, mg_send, mg_recv)

    for load in loads[:3]:
        load.wait()
    scatter = Scatter(
        ring, part, far, near, last_far, last_near, expert_out, rs_send, rs_recv
    )
    half_rows = slots // 2
    for half in range(2):
        gather_e.finish(half)
        at = pl.ds(half * half_rows, half_rows)
        tokens = jnp.concatenate([ebuf[k // 4, k % 4, at, :] for k in range(16)], axis=1)
        opened = nt(tokens, switch_buf[...])
        opened = opened * jax.nn.sigmoid(opened)
        hidden = (opened * nt(tokens, widen_buf[...])).astype(BF16)
        for k in range(4):
            product = nn(hidden, shrink_buf[:, k * 512 : (k + 1) * 512]).astype(BF16)
            for m in range(4):
                part[k, m, at, :] = product[:, m * LANES : (m + 1) * LANES]
        scatter.start(half)

    gather_m.start()
    for m in range(4):
        scatter.pass_on(0, m)
        scatter.pass_on(1, m)
    gather_m.near()
    for m in range(4):
        scatter.collect(0, m)
        scatter.collect(1, m)
    gather_m.far()
    for half in range(2):
        scatter.last_pass(half)
    for half in range(2):
        scatter.end(half)

    def give_back(k, _):
        other, device = ep_peer(k)
        send(
            expert_out.at[pl.ds(pl.multiple_of(other * CAP, CAP), CAP), :],
            returned.at[own_slots, :],
            all_send.at[3],
            all_recv.at[3],
            device,
        )
        return _

    lax.fori_loop(1, ep_count, give_back, 0)
    returned[own_slots, :] = expert_out[own_slots, :]

    for n in range(4):
        gather_m.relay(n)
    loads[3].wait()
    all_arrived(emit_buf.at[pl.ds(0, 15 * LANES), :], 4)
    for half in range(2):
        gather_m.finish(half)
        at = pl.ds(half * (tok // 2), tok // 2)
        heads = jnp.concatenate([mbuf[k // 4, k % 4, at, :] for k in range(16)], axis=1)
        out_a_ref[at, :] = nn(heads, emit_buf[...]).astype(BF16)

    all_arrived(returned.at[pl.ds(0, slots - CAP), :], 3)
    results = returned[...]
    same = iota((rows_b, rows_b), 0) == iota((rows_b, rows_b), 1)
    mixed_b = jnp.zeros((rows_b, LANES), F32)
    for k in range(2):
        share = jnp.sum(jnp.where(same, shares_ref[k : k + 1, :], 0.0), axis=1, keepdims=True)
        mixed_b = mixed_b + tn(picks[k], results) * share
    out_b_ref[...] = mixed_b.astype(BF16)

    def all_sent(ref, k):
        pltpu.make_async_copy(ref, ref, all_send.at[k]).wait()

    all_sent(outgoing.at[pl.ds(0, slots - CAP), :], 0)
    all_sent(leg1_in.at[pl.ds(0, ep_count - 1)], 1)
    all_sent(leg2_in.at[pl.ds(0, ep_count - 1)], 2)
    all_sent(returned.at[pl.ds(0, slots - CAP), :], 3)
    all_sent(emit_buf.at[pl.ds(0, 15 * LANES), :], 4)
    gather_e.drain()
    gather_m.drain()
    scatter.drain()


def per_device(*args):
    (q, right, left, v, bounds, spikes, gain, emit, rows, rows_gain, ids, shares, switch, widen, shrink) = args
    ep_count = lax.axis_size("z") * 2
    tok, rows_b, width = q.shape[0], rows.shape[0], rows.shape[1]
    hidden = switch.shape[2]
    slots = ep_count * CAP
    chunks = tok // CHUNK
    z_count = ep_count // 2
    rows_s = LANES // z_count
    n, r = slots // 2, slots // 4
    vmem = pl.BlockSpec(memory_space=pltpu.VMEM)
    anywhere = pl.BlockSpec(memory_space=pl.ANY)
    dma = pltpu.SemaphoreType.DMA
    return pl.pallas_call(
        functools.partial(kernel, ep_count),
        out_shape=(
            jax.ShapeDtypeStruct((tok, LANES), BF16),
            jax.ShapeDtypeStruct((rows_b, LANES), BF16),
        ),
        in_specs=[vmem] * 7 + [anywhere] + [vmem] * 4 + [anywhere] * 3,
        out_specs=(vmem, vmem),
        scratch_shapes=[
            pltpu.VMEM((hidden, width), BF16),
            pltpu.VMEM((hidden, width), BF16),
            pltpu.VMEM((hidden, width), BF16),
            pltpu.VMEM((width, LANES), BF16),
            pltpu.VMEM((slots, LANES), BF16),
            pltpu.VMEM((4, 4, slots, LANES), BF16),
            pltpu.VMEM((4, 4, slots, LANES), BF16),
            pltpu.VMEM((2, 2, 4, r, LANES), BF16),
            pltpu.VMEM((2, 2, 4, n, LANES), BF16),
            pltpu.VMEM((2, 2, r, LANES), BF16),
            pltpu.VMEM((2, 2, n, LANES), BF16),
            pltpu.VMEM((slots, LANES), BF16),
            pltpu.VMEM((slots, LANES), BF16),
            pltpu.VMEM((2, slots, rows_b), BF16),
            pltpu.VMEM((tok, LANES), F32),
            pltpu.VMEM((tok, LANES), BF16),
            pltpu.VMEM((tok, LANES), BF16),
            pltpu.VMEM((chunks, LANES, LANES), F32),
            pltpu.VMEM((chunks, LANES, LANES), F32),
            pltpu.VMEM((2, chunks, 1, LANES), F32),
            pltpu.VMEM((z_count, 2, rows_s + 8, LANES), BF16),
            pltpu.VMEM((ep_count, rows_s + 8, LANES), BF16),
            pltpu.VMEM((ep_count, rows_s, LANES), BF16),
            pltpu.VMEM((ep_count, rows_s, LANES), BF16),
            pltpu.VMEM((4, 4, tok, LANES), BF16),
            dma((4,)),
            dma((5,)),
            dma((5,)),
            dma((2, 20)),
            dma((2, 20)),
            dma((2, 20)),
            dma((2, 20)),
            dma((2, 20)),
            dma((2, 20)),
        ],
        compiler_params=pltpu.CompilerParams(collective_id=0, has_side_effects=True),
    )(
        q,
        right,
        left,
        v,
        bounds,
        spikes,
        gain.reshape(1, -1),
        emit,
        rows,
        rows_gain.reshape(1, -1),
        ids.T,
        shares.T,
        switch.transpose(0, 2, 1),
        widen.transpose(0, 2, 1),
        shrink,
    )


def solution(mesh):
    ep, tp = mesh.shape["ep"], mesh.shape["tp"]
    split = Mesh(mesh.devices.reshape(ep // 2, 2, tp // 4, 4), ("z", "c", "y", "x"))
    e, f = ("z", "c"), ("y", "x")
    return jax.shard_map(
        per_device,
        mesh=split,
        in_specs=(
            P(e, f),
            P(e, f),
            P(e, f),
            P(e, f),
            P(None, f),
            P(f, e),
            P(f),
            P(f, None),
            P(e, None),
            P(),
            P(e, None),
            P(e, None),
            P(e, None, f),
            P(e, None, f),
            P(e, f, None),
        ),
        out_specs=(P(e, f), P(e, f)),
        check_vma=False,
    )
```

```python
import functools

import jax
import jax.numpy as jnp
from jax import lax
from jax.experimental import pallas as pl
from jax.experimental.pallas import tpu as pltpu
from jax.sharding import Mesh
from jax.sharding import PartitionSpec as P

EPS = 1e-06
CAP = 16
LANES = 128
CHUNK = 128
DIRECT_GATHER = (False, True)
DIRECT_SCATTER = (False, False)
MESH = pl.DeviceIdType.MESH
F32 = jnp.float32
BF16 = jnp.bfloat16


def nn(a, b):
    return lax.dot_general(a, b, (((1,), (0,)), ((), ())), preferred_element_type=F32)


def nt(a, b):
    return lax.dot_general(a, b, (((1,), (1,)), ((), ())), preferred_element_type=F32)


def tn(a, b):
    return lax.dot_general(a, b, (((0,), (0,)), ((), ())), preferred_element_type=F32)


def iota(shape, dim):
    return lax.broadcasted_iota(jnp.int32, shape, dim)


def three_parts(a):
    hi = a.astype(BF16).astype(F32)
    rest = a - hi
    mid = rest.astype(BF16).astype(F32)
    return hi, mid, (rest - mid).astype(BF16).astype(F32)


def send(src, dst, send_sem, recv_sem, device):
    copy = pltpu.make_async_remote_copy(
        src_ref=src,
        dst_ref=dst,
        send_sem=send_sem,
        recv_sem=recv_sem,
        device_id=device,
        device_id_type=MESH,
    )
    copy.start()
    return copy


class Ring:
    def __init__(self, z, c, y, x):
        self.z, self.c, self.y, self.x = z, c, y, x

    def along(self, axis, step):
        return lax.rem((self.x if axis == 0 else self.y) + step, 4)

    def device(self, axis, step):
        there = self.along(axis, step)
        return (self.z, self.c, self.y, there) if axis == 0 else (self.z, self.c, there, self.x)


class Gather:
    ORDER = (0, 3, 1, 2)

    def __init__(self, ring, buf, base, rows, direct, send_sems, recv_sems):
        self.ring, self.buf, self.base, self.rows, self.direct = ring, buf, base, rows, direct
        self.send_sems, self.recv_sems = send_sems, recv_sems
        self.sent = []

    def block(self, half, first, second, part):
        a, b = self.ring.along(half, first), self.ring.along(1 - half, second)
        y, x = (b, a) if half == 0 else (a, b)
        n = self.rows // 2
        start, size = {None: (0, n), 0: (0, n // 2), 1: (n // 2, n // 2)}[part]
        return self.buf.at[y, x, pl.ds(self.base + half * n + start, size), :]

    def go(self, half, axis, step, block, k):
        self.sent.append(
            send(
                block,
                block,
                self.send_sems.at[half, k],
                self.recv_sems.at[half, k],
                self.ring.device(axis, step),
            )
        )

    def arrived(self, half, block, k):
        pltpu.make_async_copy(block, block, self.recv_sems.at[half, k]).wait()

    def second(self, half, n):
        first = self.ORDER[n]
        block = self.block(half, first, 0, None)
        self.go(half, 1 - half, 1, block, 4 + 4 * n)
        self.go(half, 1 - half, 3, block, 5 + 4 * n)
        if self.direct:
            self.go(half, 1 - half, 2, block, 6 + 4 * n)

    def start(self):
        for half in range(2):
            block = self.block(half, 0, 0, None)
            self.go(half, half, 1, block, 0)
            self.go(half, half, 3, block, 1)
            self.go(half, half, 2, block, 2)
        for half in range(2):
            self.second(half, 0)

    def near(self):
        for half in range(2):
            self.arrived(half, self.block(half, 3, 0, None), 0)
            self.second(half, 1)
            self.arrived(half, self.block(half, 1, 0, None), 1)
            self.second(half, 2)

    def far(self):
        for half in range(2):
            self.arrived(half, self.block(half, 2, 0, None), 2)
            self.second(half, 3)

    def relay(self, n):
        first = self.ORDER[n]
        for half in () if self.direct else range(2):
            self.arrived(half, self.block(half, first, 3, None), 4 + 4 * n)
            self.go(half, 1 - half, 1, self.block(half, first, 3, 0), 6 + 4 * n)
            self.arrived(half, self.block(half, first, 1, None), 5 + 4 * n)
            self.go(half, 1 - half, 3, self.block(half, first, 1, 1), 7 + 4 * n)

    def finish(self, half):
        for n in range(4):
            first = self.ORDER[n]
            if self.direct:
                self.arrived(half, self.block(half, first, 3, None), 4 + 4 * n)
                self.arrived(half, self.block(half, first, 1, None), 5 + 4 * n)
                self.arrived(half, self.block(half, first, 2, None), 6 + 4 * n)
            else:
                self.arrived(half, self.block(half, first, 2, 0), 6 + 4 * n)
                self.arrived(half, self.block(half, first, 2, 1), 7 + 4 * n)

    def drain(self):
        for copy in self.sent:
            copy.wait_send()


class Scatter:
    ORDER = (2, 1, 3, 0)

    def __init__(self, ring, part, base, rows, direct, far, near, last, out, send_sems, recv_sems):
        self.ring, self.part, self.base, self.direct, self.out = ring, part, base, direct, out
        self.far, self.near, self.last = far, near, last
        self.send_sems, self.recv_sems = send_sems, recv_sems
        self.n = rows // 2
        self.sent = []

    def block(self, half, first, second, lo, size):
        axis = 1 - half
        a, b = self.ring.along(axis, first), self.ring.along(1 - axis, second)
        y, x = (a, b) if axis == 1 else (b, a)
        return self.part.at[y, x, pl.ds(self.base + half * self.n + lo, size), :]

    def go(self, half, axis, step, src, dst, k):
        self.sent.append(
            send(
                src,
                dst,
                self.send_sems.at[half, k],
                self.recv_sems.at[half, k],
                self.ring.device(axis, step),
            )
        )

    def arrived(self, half, ref, k):
        pltpu.make_async_copy(ref, ref, self.recv_sems.at[half, k]).wait()

    def start(self, half):
        q = self.n // 2
        for m in range(4):
            o = self.ORDER[m]
            if self.direct:
                for way, step in ((0, 1), (1, 3)):
                    src = self.block(half, step, o, 0, self.n)
                    self.go(half, 1 - half, step, src, self.near.at[half, way, m], 4 * m + 2 + way)
                src = self.block(half, 2, o, 0, self.n)
                self.go(half, 1 - half, 2, src, self.far.at[half, m], 4 * m)
            else:
                for way, step in ((0, 1), (1, 3)):
                    src = self.block(half, 2, o, way * q, q)
                    dst = self.far.at[half, m, pl.ds(way * q, q), :]
                    self.go(half, 1 - half, step, src, dst, 4 * m + way)

    def pass_on(self, half, m):
        q, o = self.n // 2, self.ORDER[m]
        for way, step in () if self.direct else ((0, 1), (1, 3)):
            come = self.far.at[half, m, pl.ds(way * q, q), :]
            self.arrived(half, come, 4 * m + way)
            mine = self.block(half, step, o, way * q, q)
            mine[...] = (mine[...].astype(F32) + come[...].astype(F32)).astype(BF16)
            self.go(
                half,
                1 - half,
                step,
                self.block(half, step, o, 0, self.n),
                self.near.at[half, way, m],
                4 * m + 2 + way,
            )

    def collect(self, half, m):
        o = self.ORDER[m]
        for way in range(2):
            self.arrived(half, self.near.at[half, way, m], 4 * m + 2 + way)
        mine = self.block(half, 0, o, 0, self.n)
        total = mine[...].astype(F32) + self.near[half, 0, m].astype(F32)
        total = total + self.near[half, 1, m].astype(F32)
        if self.direct:
            self.arrived(half, self.far.at[half, m], 4 * m)
            total = total + self.far[half, m].astype(F32)
        mine[...] = total.astype(BF16)
        if m < 3:
            self.go(half, half, o, mine, self.last.at[half, m], 16 + m)

    def end(self, half):
        total = self.block(half, 0, 0, 0, self.n)[...].astype(F32)
        for m in (1, 2, 0):
            self.arrived(half, self.last.at[half, m], 16 + m)
            total = total + self.last[half, m].astype(F32)
        self.out[pl.ds(self.base + half * self.n, self.n), :] = total.astype(BF16)

    def drain(self):
        for copy in self.sent:
            copy.wait_send()


def kernel(
    ep_count,
    q_hbm,
    right_hbm,
    left_hbm,
    v_hbm,
    bounds_hbm,
    spikes_hbm,
    gain_hbm,
    emit_ref,
    rows_hbm,
    rows_gain_hbm,
    ids_hbm,
    shares_hbm,
    switch_ref,
    widen_ref,
    shrink_ref,
    out_a_ref,
    out_b_ref,
    q_ref,
    right_ref,
    left_ref,
    v_ref,
    bounds_ref,
    spikes_ref,
    gain_ref,
    rows_ref,
    rows_gain_ref,
    ids_ref,
    shares_ref,
    switch_buf,
    widen_buf,
    shrink_buf,
    emit_a,
    emit_b,
    outgoing,
    ebuf,
    part,
    far,
    near,
    last,
    expert_out,
    returned,
    picks,
    intra,
    query_f,
    query_b,
    added_f,
    added_b,
    chunk_decay,
    leg1_out,
    leg1_in,
    leg2_out,
    leg2_in,
    mixed_in,
    mixed_part,
    mixed_come,
    load_sems,
    all_send,
    all_recv,
    eg_send,
    eg_recv,
    m_send,
    m_recv,
    rs_send,
    rs_recv,
):
    z, c = lax.axis_index("z"), lax.axis_index("c")
    y, x = lax.axis_index("y"), lax.axis_index("x")
    s, t = 2 * z + c, 4 * y + x
    ring = Ring(z, c, y, x)
    tok = q_ref.shape[0]
    chunks = tok // CHUNK
    rows_b = rows_ref.shape[0]
    slots = ep_count * CAP
    near_count = ep_count // 2
    shift = ep_count // 4

    def ep_peer(k):
        other = lax.rem(s + k, ep_count)
        return other, (lax.div(other, 2), lax.rem(other, 2), y, x)

    columns = pl.ds(pl.multiple_of(t * LANES, LANES), LANES)

    def far_columns(_, to):
        return pl.ds(pl.multiple_of(to * (4 * LANES), 4 * LANES), 4 * LANES)

    def near_columns(k, to):
        return pl.ds(pl.multiple_of((4 * k + to) * LANES, LANES), LANES)

    def near_place(k):
        return pl.ds(k * LANES, LANES)

    core_rows = pl.ds(pl.multiple_of(c * (LANES // 2), LANES // 2), LANES // 2)
    loads = [
        pltpu.make_async_copy(src, dst, load_sems.at[i])
        for i, (src, dst) in enumerate(
            (
                (ids_hbm, ids_ref),
                (rows_hbm, rows_ref),
                (rows_gain_hbm, rows_gain_ref),
                (bounds_hbm, bounds_ref),
                (spikes_hbm, spikes_ref),
                (q_hbm, q_ref),
                (right_hbm, right_ref),
                (left_hbm, left_ref),
                (v_hbm, v_ref),
                (gain_hbm, gain_ref),
                (shares_hbm, shares_ref),
                (switch_ref.at[0], switch_buf),
                (widen_ref.at[0], widen_buf),
                (shrink_ref.at[0], shrink_buf),
                (emit_ref.at[core_rows, far_columns(0, y)], emit_b.at[y, core_rows, :]),
                *(
                    (emit_ref.at[core_rows, near_columns(k, x)], emit_a.at[x, core_rows, near_place(k)])
                    for k in range(4)
                ),
            )
        )
    ]
    for load in loads:
        load.start()
    barrier = pltpu.get_barrier_semaphore()

    def greet(k):
        pl.semaphore_signal(barrier, inc=1, device_id=ep_peer(k)[1], device_id_type=MESH)

    def greet_ep(k, _):
        greet(near_count - k)
        greet(near_count + k)
        return _

    greet(near_count)
    lax.fori_loop(1, near_count, greet_ep, 0)
    for axis in range(2):
        for step in range(1, 4):
            pl.semaphore_signal(
                barrier, inc=1, device_id=ring.device(axis, step), device_id_type=MESH
            )

    for load in loads[:3]:
        load.wait()

    width = rows_ref.shape[1]
    square = jnp.zeros((rows_b, LANES), F32)
    for k in range(width // LANES):
        piece = rows_ref[:, k * LANES : (k + 1) * LANES].astype(F32)
        square = square + piece * piece
    mean = jnp.sum(square, axis=1, keepdims=True) / width
    normed = rows_ref[:, columns].astype(F32) * lax.rsqrt(mean + EPS)
    normed = (normed * rows_gain_ref[:, columns]).astype(BF16)
    experts = iota((ep_count, rows_b), 0)
    pick0 = ids_ref[0:1, :] == experts
    pick1 = ids_ref[1:2, :] == experts
    named = (pick0 | pick1).astype(F32).astype(BF16)
    earlier = (iota((rows_b, rows_b), 0) < iota((rows_b, rows_b), 1)).astype(F32).astype(BF16)
    rank = nn(named, earlier)
    at_slot = rank.astype(jnp.int32)[:, None, :] == iota((ep_count, CAP, rows_b), 1)
    ones = jnp.where(at_slot, 1.0, 0.0)
    for k, pick in enumerate((pick0, pick1)):
        chosen = ones * jnp.where(pick, 1.0, 0.0)[:, None, :]
        picks[k] = chosen.reshape(slots, rows_b).astype(BF16)
    outgoing[...] = nn(picks[0] + picks[1], normed).astype(BF16)
    own_slots = pl.ds(pl.multiple_of(s * CAP, CAP), CAP)
    ebuf[y, x, shift * CAP : (shift + 1) * CAP, :] = outgoing[own_slots, :]

    pl.semaphore_wait(barrier, ep_count - 1 + 6)

    def dispatch(group):
        def one(k, _):
            other, device = ep_peer(k)
            place = lax.rem(shift - k + ep_count, ep_count)
            send(
                outgoing.at[pl.ds(pl.multiple_of(other * CAP, CAP), CAP), :],
                ebuf.at[y, x, pl.ds(pl.multiple_of(place * CAP, CAP), CAP), :],
                all_send.at[group],
                all_recv.at[group],
                device,
            )
            return _

        return one

    def leg1(k, _):
        other, device = ep_peer(k)
        send(
            leg1_out.at[lax.div(other, 2), lax.rem(other, 2)],
            leg1_in.at[s],
            all_send.at[2],
            all_recv.at[2],
            device,
        )
        return _

    def leg2(k, _):
        other, device = ep_peer(k)
        send(leg2_out.at[other], leg2_in.at[s], all_send.at[3], all_recv.at[3], device)
        return _

    def deal():
        for step in range(1, 4):
            for k in range(4):
                send(
                    emit_ref.at[core_rows, near_columns(k, ring.along(0, step))],
                    emit_a.at[x, core_rows, near_place(k)],
                    all_send.at[4],
                    all_recv.at[4],
                    ring.device(0, step),
                )
            send(
                emit_ref.at[core_rows, far_columns(0, ring.along(1, step))],
                emit_b.at[y, core_rows, :],
                all_send.at[7],
                all_recv.at[7],
                ring.device(1, step),
            )

    def give_back(k, _):
        other, device = ep_peer(k)
        place = lax.rem(shift + k, ep_count)
        send(
            expert_out.at[pl.ds(pl.multiple_of(place * CAP, CAP), CAP), :],
            returned.at[own_slots, :],
            all_send.at[5],
            all_recv.at[5],
            device,
        )
        return _

    def all_arrived(ref, k):
        pltpu.make_async_copy(ref, ref, all_recv.at[k]).wait()

    def all_sent(ref, k):
        pltpu.make_async_copy(ref, ref, all_send.at[k]).wait()

    near_slots = outgoing.at[pl.ds(0, (near_count - 1) * CAP), :]
    far_slots = outgoing.at[pl.ds(0, near_count * CAP), :]
    others_slots = outgoing.at[pl.ds(0, slots - CAP), :]
    rows = slots // 2
    gather = [Gather(ring, ebuf, p * rows, rows, DIRECT_GATHER[p], eg_send.at[p], eg_recv.at[p]) for p in range(2)]
    scatter = [
        Scatter(
            ring,
            part,
            p * rows,
            rows,
            DIRECT_SCATTER[p],
            far.at[p],
            near.at[p],
            last.at[p],
            expert_out,
            rs_send.at[p],
            rs_recv.at[p],
        )
        for p in range(2)
    ]

    def experts_of(p):
        at = pl.ds(p * rows, rows)
        tokens = jnp.concatenate([ebuf[k // 4, k % 4, at, :] for k in range(16)], axis=1)
        opened = nt(tokens, switch_buf[...])
        opened = opened * jax.nn.sigmoid(opened)
        hidden = (opened * nt(tokens, widen_buf[...])).astype(BF16)
        for k in range(4):
            product = nn(hidden, shrink_buf[:, k * 512 : (k + 1) * 512]).astype(BF16)
            for m in range(4):
                part[k, m, at, :] = product[:, m * LANES : (m + 1) * LANES]

    lax.fori_loop(1, shift + 1, dispatch(0), 0)
    lax.fori_loop(ep_count - shift + 1, ep_count, dispatch(0), 0)
    lax.fori_loop(shift + 1, ep_count - shift + 1, dispatch(1), 0)
    deal()

    for load in loads[3:9]:
        load.wait()
    tri = iota((CHUNK, CHUNK), 0) >= iota((CHUNK, CHUNK), 1)
    tri_t = iota((CHUNK, CHUNK), 0) <= iota((CHUNK, CHUNK), 1)
    for n in range(chunks):
        at = slice(n * CHUNK, (n + 1) * CHUNK)
        query = q_ref[at, :].astype(F32)
        query = query * jax.nn.sigmoid(query)
        values = v_ref[at, :]
        spike = spikes_ref[0:1, at]
        scores = []
        for d, (pre_ref, mask, queries, added) in enumerate(
            ((right_ref, tri, query_f, added_f), (left_ref, tri_t, query_b, added_b))
        ):
            pre = pre_ref[at, :].astype(F32)
            bound = bounds_ref[d : d + 1, :]
            gap = 1.0 - bound
            log_decay = jnp.log(bound + gap * jax.nn.sigmoid(pre))
            key = gap * jax.nn.sigmoid(-pre)
            split = jnp.concatenate(three_parts(log_decay), axis=1).astype(BF16)
            summed = nn(jnp.where(mask, 1.0, 0.0).astype(BF16), split)
            total = summed[:, :LANES] + summed[:, LANES : 2 * LANES] + summed[:, 2 * LANES :]
            total = total + jnp.sum(jnp.where(mask, spike, 0.0), axis=1, keepdims=True)
            whole = total[CHUNK - 1 : CHUNK, :] if d == 0 else total[0:1, :]
            middle = total[CHUNK // 2 : CHUNK // 2 + 1, :]
            near_q = (query * jnp.exp(total - middle)).astype(BF16)
            near_k = (key * jnp.exp(middle - total)).astype(BF16)
            scores.append(jnp.where(mask, nt(near_q, near_k), 0.0))
            queries[at, :] = (query * jnp.exp(total)).astype(BF16)
            added[n] = tn(values, (key * jnp.exp(whole - total)).astype(BF16))
            chunk_decay[d, n] = whole
        intra[at, :] = nn((scores[0] + scores[1]).astype(BF16), values)

    z_count = ep_count // 2
    rows_s = LANES // z_count
    for d, (added, order) in enumerate(
        ((added_f, range(chunks)), (added_b, range(chunks - 1, -1, -1)))
    ):
        state, decay = None, None
        for n in order:
            state = added[n] if state is None else state * jnp.exp(chunk_decay[d, n]) + added[n]
            decay = chunk_decay[d, n] if decay is None else decay + chunk_decay[d, n]
        hi, mid, lo = three_parts(decay)
        row = iota((8, LANES), 0)
        tail = jnp.where(row == 0, hi, jnp.where(row == 1, mid, jnp.where(row == 2, lo, 0.0)))
        tail = jnp.broadcast_to(tail[None], (z_count, 8, LANES))
        leg1_out[:, d] = jnp.concatenate(
            [state.reshape(z_count, rows_s, LANES), tail], axis=1
        ).astype(BF16)
    leg1_in[s] = leg1_out[z, c]
    all_arrived(near_slots, 0)
    gather[0].start()
    gather[0].near()
    gather[0].far()
    lax.fori_loop(1, ep_count, leg1, 0)
    gather[0].relay(0)
    all_arrived(far_slots, 1)
    gather[1].start()
    gather[0].relay(1)
    gather[0].relay(2)
    gather[0].relay(3)
    gather[1].near()
    gather[1].far()
    gather[1].relay(0)
    gather[1].relay(1)
    gather[1].relay(2)
    gather[1].relay(3)
    for load in loads[14:19]:
        load.wait()
    dealt = emit_a.at[pl.ds(0, 3), pl.ds(0, LANES // 2), :]
    all_arrived(dealt, 4)
    all_arrived(dealt, 7)
    for emit, k in ((emit_a, 6), (emit_b, 8)):
        block = emit.at[:, core_rows, :]
        send(block, block, all_send.at[k], all_recv.at[k], (z, 1 - c, y, x))
    all_arrived(leg1_in.at[pl.ds(0, ep_count - 1)], 2)
    carried = jnp.zeros((rows_s, LANES), F32)
    for n in range(ep_count):
        i = jnp.where(c == 0, n, ep_count - 1 - n)
        tile = leg1_in[i].astype(F32)
        leg2_out[i] = carried.astype(BF16)
        decay = tile[rows_s : rows_s + 1] + tile[rows_s + 1 : rows_s + 2] + tile[rows_s + 2 : rows_s + 3]
        carried = carried * jnp.exp(decay) + tile[:rows_s]
    lax.fori_loop(1, ep_count, leg2, 0)
    leg2_in[s] = leg2_out[s]
    for half in range(2):
        gather[0].finish(half)
    for load in loads[11:14]:
        load.wait()
    experts_of(0)
    for half in range(2):
        scatter[0].start(half)
    for half in range(2):
        gather[1].finish(half)
    experts_of(1)
    for half in range(2):
        scatter[1].start(half)
    for m in range(4):
        for half in range(2):
            scatter[0].pass_on(half, m)
    for m in range(4):
        for half in range(2):
            scatter[1].pass_on(half, m)
    for m in range(4):
        for half in range(2):
            scatter[0].collect(half, m)
    all_arrived(leg2_in.at[pl.ds(0, ep_count - 1)], 3)
    loads[9].wait()
    entries = [
        jnp.concatenate([leg2_in[2 * k + d].astype(F32) for k in range(z_count)], axis=0)
        for d in range(2)
    ]
    for d, (added, queries, order) in enumerate(
        ((added_f, query_f, range(chunks)), (added_b, query_b, range(chunks - 1, -1, -1)))
    ):
        state = entries[d]
        for n in order:
            at = slice(n * CHUNK, (n + 1) * CHUNK)
            intra[at, :] += nt(queries[at, :], state.astype(BF16))
            state = state * jnp.exp(chunk_decay[d, n]) + added[n]
    mixed = intra[...]
    mixed = mixed * lax.rsqrt(jnp.mean(mixed * mixed, axis=1, keepdims=True) + EPS)
    mixed = (mixed * gain_ref[...]).astype(BF16)
    mixed_in[0, x] = mixed[: tok // 2]
    mixed_in[1, y] = mixed[tok // 2 :]
    flows_m = []
    for half in range(2):
        own = mixed_in.at[half, (x, y)[half]]
        for step in range(1, 4):
            flows_m.append(
                send(own, own, m_send.at[0, half, step], m_recv.at[0, half, step], ring.device(half, step))
            )
    for m in range(4):
        for half in range(2):
            scatter[1].collect(half, m)
    for half in range(2):
        scatter[0].end(half)
    lax.fori_loop(1, near_count - shift, give_back, 0)
    lax.fori_loop(ep_count - shift, ep_count, give_back, 0)
    returned[own_slots, :] = expert_out[shift * CAP : (shift + 1) * CAP, :]
    for half in range(2):
        scatter[1].end(half)
    lax.fori_loop(near_count - shift, ep_count - shift, give_back, 0)
    whole = emit_a.at[:, pl.ds(0, LANES // 2), :]
    all_arrived(whole, 6)
    all_arrived(whole, 8)
    for half in range(2):
        for step in range(1, 4):
            come = mixed_in.at[half, ring.along(half, step)]
            pltpu.make_async_copy(come, come, m_recv.at[0, half, step]).wait()
        heads = jnp.concatenate([mixed_in[half, k] for k in range(4)], axis=1)
        emit = (emit_a, emit_b)[half][...].reshape(4 * LANES, 4 * LANES)
        product = nn(heads, emit)
        for k in range(4):
            mixed_part[half, k] = product[:, k * LANES : (k + 1) * LANES].astype(BF16)
        for step in range(1, 4):
            flows_m.append(
                send(
                    mixed_part.at[half, ring.along(1 - half, step)],
                    mixed_come.at[half, step],
                    m_send.at[1, half, step],
                    m_recv.at[1, half, step],
                    ring.device(1 - half, step),
                )
            )
    for half in range(2):
        total = mixed_part[half, (y, x)[half]].astype(F32)
        for step in range(1, 4):
            come = mixed_come.at[half, step]
            pltpu.make_async_copy(come, come, m_recv.at[1, half, step]).wait()
            total = total + mixed_come[half, step].astype(F32)
        out_a_ref[half * (tok // 2) : (half + 1) * (tok // 2), :] = total.astype(BF16)
    all_arrived(others_slots, 5)
    loads[10].wait()
    results = returned[...]
    same = iota((rows_b, rows_b), 0) == iota((rows_b, rows_b), 1)
    mixed_b = jnp.zeros((rows_b, LANES), F32)
    for k in range(2):
        share = jnp.sum(jnp.where(same, shares_ref[k : k + 1, :], 0.0), axis=1, keepdims=True)
        mixed_b = mixed_b + tn(picks[k], results) * share
    out_b_ref[...] = mixed_b.astype(BF16)

    all_sent(near_slots, 0)
    all_sent(far_slots, 1)
    all_sent(leg1_in.at[pl.ds(0, ep_count - 1)], 2)
    all_sent(leg2_in.at[pl.ds(0, ep_count - 1)], 3)
    for k in (4, 7):
        all_sent(dealt, k)
    for k in (6, 8):
        all_sent(whole, k)
    for copy in flows_m:
        copy.wait_send()
    all_sent(others_slots, 5)
    for flow in (*gather, *scatter):
        flow.drain()


def per_device(*args):
    (q, right, left, v, bounds, spikes, gain, emit, rows, rows_gain, ids, shares, switch, widen, shrink) = args
    ep_count = lax.axis_size("z") * 2
    tok, rows_b, width = q.shape[0], rows.shape[0], rows.shape[1]
    hidden = switch.shape[2]
    slots = ep_count * CAP
    chunks = tok // CHUNK
    z_count = ep_count // 2
    rows_s = LANES // z_count
    n = slots // 4
    dma = pltpu.SemaphoreType.DMA
    return pl.pallas_call(
        functools.partial(kernel, ep_count),
        out_shape=(
            pltpu.VMEM((tok, LANES), BF16),
            pltpu.VMEM((rows_b, LANES), BF16),
        ),
        in_specs=[pl.BlockSpec(memory_space=pl.ANY)] * 15,
        out_specs=(pl.BlockSpec(memory_space=pltpu.VMEM),) * 2,
        scratch_shapes=[
            pltpu.VMEM((tok, LANES), BF16),
            pltpu.VMEM((tok, LANES), BF16),
            pltpu.VMEM((tok, LANES), BF16),
            pltpu.VMEM((tok, LANES), BF16),
            pltpu.VMEM((2, LANES), F32),
            pltpu.VMEM((1, tok), F32),
            pltpu.VMEM((1, LANES), F32),
            pltpu.VMEM((rows_b, width), BF16),
            pltpu.VMEM((1, width), F32),
            pltpu.VMEM((2, rows_b), jnp.int32),
            pltpu.VMEM((2, rows_b), F32),
            pltpu.VMEM((hidden, width), BF16),
            pltpu.VMEM((hidden, width), BF16),
            pltpu.VMEM((hidden, width), BF16),
            pltpu.VMEM((4, LANES, 4 * LANES), BF16),
            pltpu.VMEM((4, LANES, 4 * LANES), BF16),
            pltpu.VMEM((slots, LANES), BF16),
            pltpu.VMEM((4, 4, slots, LANES), BF16),
            pltpu.VMEM((4, 4, slots, LANES), BF16),
            pltpu.VMEM((2, 2, 4, n, LANES), BF16),
            pltpu.VMEM((2, 2, 2, 4, n, LANES), BF16),
            pltpu.VMEM((2, 2, 3, n, LANES), BF16),
            pltpu.VMEM((slots, LANES), BF16),
            pltpu.VMEM((slots, LANES), BF16),
            pltpu.VMEM((2, slots, rows_b), BF16),
            pltpu.VMEM((tok, LANES), F32),
            pltpu.VMEM((tok, LANES), BF16),
            pltpu.VMEM((tok, LANES), BF16),
            pltpu.VMEM((chunks, LANES, LANES), F32),
            pltpu.VMEM((chunks, LANES, LANES), F32),
            pltpu.VMEM((2, chunks, 1, LANES), F32),
            pltpu.VMEM((z_count, 2, rows_s + 8, LANES), BF16),
            pltpu.VMEM((ep_count, rows_s + 8, LANES), BF16),
            pltpu.VMEM((ep_count, rows_s, LANES), BF16),
            pltpu.VMEM((ep_count, rows_s, LANES), BF16),
            pltpu.VMEM((2, 4, tok // 2, LANES), BF16),
            pltpu.VMEM((2, 4, tok // 2, LANES), BF16),
            pltpu.VMEM((2, 4, tok // 2, LANES), BF16),
            dma((19,)),
            dma((9,)),
            dma((9,)),
            dma((2, 2, 20)),
            dma((2, 2, 20)),
            dma((2, 2, 4)),
            dma((2, 2, 4)),
            dma((2, 2, 20)),
            dma((2, 2, 20)),
        ],
        compiler_params=pltpu.CompilerParams(collective_id=0, has_side_effects=True),
    )(
        q,
        right,
        left,
        v,
        bounds,
        spikes,
        gain.reshape(1, -1),
        emit,
        rows,
        rows_gain.reshape(1, -1),
        ids.T,
        shares.T,
        switch.transpose(0, 2, 1),
        widen.transpose(0, 2, 1),
        shrink,
    )


def solution(mesh):
    ep, tp = mesh.shape["ep"], mesh.shape["tp"]
    split = Mesh(mesh.devices.reshape(ep // 2, 2, tp // 4, 4), ("z", "c", "y", "x"))
    e, f = ("z", "c"), ("y", "x")
    return jax.shard_map(
        per_device,
        mesh=split,
        in_specs=(
            P(e, f),
            P(e, f),
            P(e, f),
            P(e, f),
            P(None, f),
            P(f, e),
            P(f),
            P(f, None),
            P(e, None),
            P(),
            P(e, None),
            P(e, None),
            P(e, None, f),
            P(e, None, f),
            P(e, f, None),
        ),
        out_specs=(P(e, f), P(e, f)),
        check_vma=False,
    )
```

```python
import functools

import jax
import jax.numpy as jnp
from jax import lax
from jax.experimental import pallas as pl
from jax.experimental.pallas import tpu as pltpu
from jax.sharding import Mesh
from jax.sharding import PartitionSpec as P

EPS = 1e-06
CAP = 16
LANES = 128
CHUNK = 128
DIRECT_GATHER = (False, True)
DIRECT_SCATTER = (False, False)
MESH = pl.DeviceIdType.MESH
F32 = jnp.float32
BF16 = jnp.bfloat16


def nn(a, b):
    return lax.dot_general(a, b, (((1,), (0,)), ((), ())), preferred_element_type=F32)


def nt(a, b):
    return lax.dot_general(a, b, (((1,), (1,)), ((), ())), preferred_element_type=F32)


def tn(a, b):
    return lax.dot_general(a, b, (((0,), (0,)), ((), ())), preferred_element_type=F32)


def iota(shape, dim):
    return lax.broadcasted_iota(jnp.int32, shape, dim)


def three_parts(a):
    hi = a.astype(BF16).astype(F32)
    rest = a - hi
    mid = rest.astype(BF16).astype(F32)
    return hi, mid, (rest - mid).astype(BF16).astype(F32)


def send(src, dst, send_sem, recv_sem, device):
    copy = pltpu.make_async_remote_copy(
        src_ref=src,
        dst_ref=dst,
        send_sem=send_sem,
        recv_sem=recv_sem,
        device_id=device,
        device_id_type=MESH,
    )
    copy.start()
    return copy


class Ring:
    def __init__(self, z, c, y, x):
        self.z, self.c, self.y, self.x = z, c, y, x

    def along(self, axis, step):
        return lax.rem((self.x if axis == 0 else self.y) + step, 4)

    def device(self, axis, step):
        there = self.along(axis, step)
        return (self.z, self.c, self.y, there) if axis == 0 else (self.z, self.c, there, self.x)


class Gather:
    ORDER = (0, 3, 1, 2)

    def __init__(self, ring, buf, base, rows, direct, send_sems, recv_sems):
        self.ring, self.buf, self.base, self.rows, self.direct = ring, buf, base, rows, direct
        self.send_sems, self.recv_sems = send_sems, recv_sems
        self.sent = []

    def block(self, half, first, second, part):
        a, b = self.ring.along(half, first), self.ring.along(1 - half, second)
        y, x = (b, a) if half == 0 else (a, b)
        n = self.rows // 2
        start, size = {None: (0, n), 0: (0, n // 2), 1: (n // 2, n // 2)}[part]
        return self.buf.at[y, x, pl.ds(self.base + half * n + start, size), :]

    def go(self, half, axis, step, block, k):
        self.sent.append(
            send(
                block,
                block,
                self.send_sems.at[half, k],
                self.recv_sems.at[half, k],
                self.ring.device(axis, step),
            )
        )

    def arrived(self, half, block, k):
        pltpu.make_async_copy(block, block, self.recv_sems.at[half, k]).wait()

    def second(self, half, n):
        first = self.ORDER[n]
        block = self.block(half, first, 0, None)
        self.go(half, 1 - half, 1, block, 4 + 4 * n)
        self.go(half, 1 - half, 3, block, 5 + 4 * n)
        if self.direct:
            self.go(half, 1 - half, 2, block, 6 + 4 * n)

    def start(self):
        for half in range(2):
            block = self.block(half, 0, 0, None)
            self.go(half, half, 1, block, 0)
            self.go(half, half, 3, block, 1)
            self.go(half, half, 2, block, 2)
        for half in range(2):
            self.second(half, 0)

    def near(self):
        for half in range(2):
            self.arrived(half, self.block(half, 3, 0, None), 0)
            self.second(half, 1)
            self.arrived(half, self.block(half, 1, 0, None), 1)
            self.second(half, 2)

    def far(self):
        for half in range(2):
            self.arrived(half, self.block(half, 2, 0, None), 2)
            self.second(half, 3)

    def relay(self, n):
        first = self.ORDER[n]
        for half in () if self.direct else range(2):
            self.arrived(half, self.block(half, first, 3, None), 4 + 4 * n)
            self.go(half, 1 - half, 1, self.block(half, first, 3, 0), 6 + 4 * n)
            self.arrived(half, self.block(half, first, 1, None), 5 + 4 * n)
            self.go(half, 1 - half, 3, self.block(half, first, 1, 1), 7 + 4 * n)

    def finish(self, half):
        for n in range(4):
            first = self.ORDER[n]
            if self.direct:
                self.arrived(half, self.block(half, first, 3, None), 4 + 4 * n)
                self.arrived(half, self.block(half, first, 1, None), 5 + 4 * n)
                self.arrived(half, self.block(half, first, 2, None), 6 + 4 * n)
            else:
                self.arrived(half, self.block(half, first, 2, 0), 6 + 4 * n)
                self.arrived(half, self.block(half, first, 2, 1), 7 + 4 * n)

    def drain(self):
        for copy in self.sent:
            copy.wait_send()


class Scatter:
    ORDER = (2, 1, 3, 0)

    def __init__(self, ring, part, base, rows, direct, far, near, last, out, send_sems, recv_sems):
        self.ring, self.part, self.base, self.direct, self.out = ring, part, base, direct, out
        self.far, self.near, self.last = far, near, last
        self.send_sems, self.recv_sems = send_sems, recv_sems
        self.n = rows // 2
        self.sent = []

    def block(self, half, first, second, lo, size):
        axis = 1 - half
        a, b = self.ring.along(axis, first), self.ring.along(1 - axis, second)
        y, x = (a, b) if axis == 1 else (b, a)
        return self.part.at[y, x, pl.ds(self.base + half * self.n + lo, size), :]

    def go(self, half, axis, step, src, dst, k):
        self.sent.append(
            send(
                src,
                dst,
                self.send_sems.at[half, k],
                self.recv_sems.at[half, k],
                self.ring.device(axis, step),
            )
        )

    def arrived(self, half, ref, k):
        pltpu.make_async_copy(ref, ref, self.recv_sems.at[half, k]).wait()

    def start(self, half):
        q = self.n // 2
        for m in range(4):
            o = self.ORDER[m]
            if self.direct:
                for way, step in ((0, 1), (1, 3)):
                    src = self.block(half, step, o, 0, self.n)
                    self.go(half, 1 - half, step, src, self.near.at[half, way, m], 4 * m + 2 + way)
                src = self.block(half, 2, o, 0, self.n)
                self.go(half, 1 - half, 2, src, self.far.at[half, m], 4 * m)
            else:
                for way, step in ((0, 1), (1, 3)):
                    src = self.block(half, 2, o, way * q, q)
                    dst = self.far.at[half, m, pl.ds(way * q, q), :]
                    self.go(half, 1 - half, step, src, dst, 4 * m + way)

    def pass_on(self, half, m):
        q, o = self.n // 2, self.ORDER[m]
        for way, step in () if self.direct else ((0, 1), (1, 3)):
            come = self.far.at[half, m, pl.ds(way * q, q), :]
            self.arrived(half, come, 4 * m + way)
            mine = self.block(half, step, o, way * q, q)
            mine[...] = (mine[...].astype(F32) + come[...].astype(F32)).astype(BF16)
            self.go(
                half,
                1 - half,
                step,
                self.block(half, step, o, 0, self.n),
                self.near.at[half, way, m],
                4 * m + 2 + way,
            )

    def collect(self, half, m):
        o = self.ORDER[m]
        for way in range(2):
            self.arrived(half, self.near.at[half, way, m], 4 * m + 2 + way)
        mine = self.block(half, 0, o, 0, self.n)
        total = mine[...].astype(F32) + self.near[half, 0, m].astype(F32)
        total = total + self.near[half, 1, m].astype(F32)
        if self.direct:
            self.arrived(half, self.far.at[half, m], 4 * m)
            total = total + self.far[half, m].astype(F32)
        mine[...] = total.astype(BF16)
        if m < 3:
            self.go(half, half, o, mine, self.last.at[half, m], 16 + m)

    def end(self, half):
        total = self.block(half, 0, 0, 0, self.n)[...].astype(F32)
        for m in (1, 2, 0):
            self.arrived(half, self.last.at[half, m], 16 + m)
            total = total + self.last[half, m].astype(F32)
        self.out[pl.ds(self.base + half * self.n, self.n), :] = total.astype(BF16)

    def drain(self):
        for copy in self.sent:
            copy.wait_send()


def kernel(
    ep_count,
    q_hbm,
    right_hbm,
    left_hbm,
    v_hbm,
    bounds_hbm,
    spikes_hbm,
    gain_hbm,
    emit_ref,
    rows_hbm,
    rows_gain_hbm,
    ids_hbm,
    shares_hbm,
    switch_ref,
    widen_ref,
    shrink_ref,
    out_a_ref,
    out_b_ref,
    q_ref,
    right_ref,
    left_ref,
    v_ref,
    bounds_ref,
    spikes_ref,
    gain_ref,
    rows_ref,
    rows_gain_ref,
    ids_ref,
    shares_ref,
    switch_buf,
    widen_buf,
    shrink_buf,
    emit_a,
    emit_b,
    outgoing,
    ebuf,
    part,
    far,
    near,
    last,
    expert_out,
    returned,
    picks,
    taken,
    share_columns,
    intra,
    query_f,
    query_b,
    added_f,
    added_b,
    chunk_decay,
    leg1_out,
    leg1_in,
    leg2_out,
    leg2_in,
    mixed_in,
    mixed_part,
    mixed_come,
    load_sems,
    all_send,
    all_recv,
    eg_send,
    eg_recv,
    m_send,
    m_recv,
    rs_send,
    rs_recv,
):
    z, c = lax.axis_index("z"), lax.axis_index("c")
    y, x = lax.axis_index("y"), lax.axis_index("x")
    s, t = 2 * z + c, 4 * y + x
    ring = Ring(z, c, y, x)
    tok = q_ref.shape[0]
    chunks = tok // CHUNK
    rows_b = rows_ref.shape[0]
    slots = ep_count * CAP
    near_count = ep_count // 2
    shift = ep_count // 4

    def ep_peer(k):
        other = lax.rem(s + k, ep_count)
        return other, (lax.div(other, 2), lax.rem(other, 2), y, x)

    columns = pl.ds(pl.multiple_of(t * LANES, LANES), LANES)

    def far_columns(_, to):
        return pl.ds(pl.multiple_of(to * (4 * LANES), 4 * LANES), 4 * LANES)

    def near_columns(k, to):
        return pl.ds(pl.multiple_of((4 * k + to) * LANES, LANES), LANES)

    def near_place(k):
        return pl.ds(k * LANES, LANES)

    core_rows = pl.ds(pl.multiple_of(c * (LANES // 2), LANES // 2), LANES // 2)
    loads = [
        pltpu.make_async_copy(src, dst, load_sems.at[i])
        for i, (src, dst) in enumerate(
            (
                (ids_hbm, ids_ref),
                (rows_hbm, rows_ref),
                (rows_gain_hbm, rows_gain_ref),
                (bounds_hbm, bounds_ref),
                (spikes_hbm, spikes_ref),
                (q_hbm, q_ref),
                (right_hbm, right_ref),
                (left_hbm, left_ref),
                (v_hbm, v_ref),
                (gain_hbm, gain_ref),
                (shares_hbm, shares_ref),
                (switch_ref.at[0], switch_buf),
                (widen_ref.at[0], widen_buf),
                (shrink_ref.at[0], shrink_buf),
                (emit_ref.at[core_rows, far_columns(0, y)], emit_b.at[y, core_rows, :]),
                *(
                    (emit_ref.at[core_rows, near_columns(k, x)], emit_a.at[x, core_rows, near_place(k)])
                    for k in range(4)
                ),
            )
        )
    ]
    for load in loads:
        load.start()
    barrier = pltpu.get_barrier_semaphore()

    def greet(k):
        pl.semaphore_signal(barrier, inc=1, device_id=ep_peer(k)[1], device_id_type=MESH)

    def pairs(one, low, high, count):
        def both(i, _):
            one(low - i)
            one(high + i)
            return _

        lax.fori_loop(0, count, both, 0)

    def everyone(one):
        one(near_count)
        pairs(one, near_count - 1, near_count + 1, near_count - 1)

    everyone(greet)
    for axis in range(2):
        for step in range(1, 4):
            pl.semaphore_signal(
                barrier, inc=1, device_id=ring.device(axis, step), device_id_type=MESH
            )

    for load in loads[:3]:
        load.wait()

    width = rows_ref.shape[1]
    square = jnp.zeros((rows_b, LANES), F32)
    for k in range(width // LANES):
        piece = rows_ref[:, k * LANES : (k + 1) * LANES].astype(F32)
        square = square + piece * piece
    mean = jnp.sum(square, axis=1, keepdims=True) / width
    normed = rows_ref[:, columns].astype(F32) * lax.rsqrt(mean + EPS)
    normed = (normed * rows_gain_ref[:, columns]).astype(BF16)
    experts = iota((ep_count, rows_b), 0)
    pick0 = ids_ref[0:1, :] == experts
    pick1 = ids_ref[1:2, :] == experts
    named = (pick0 | pick1).astype(F32).astype(BF16)
    earlier = (iota((rows_b, rows_b), 0) < iota((rows_b, rows_b), 1)).astype(F32).astype(BF16)
    rank = nn(named, earlier)
    at_slot = rank.astype(jnp.int32)[:, None, :] == iota((ep_count, CAP, rows_b), 1)
    ones = jnp.where(at_slot, 1.0, 0.0)
    for k, pick in enumerate((pick0, pick1)):
        chosen = ones * jnp.where(pick, 1.0, 0.0)[:, None, :]
        picks[k] = chosen.reshape(slots, rows_b).astype(BF16)
    outgoing[...] = nn(picks[0] + picks[1], normed).astype(BF16)
    own_slots = pl.ds(pl.multiple_of(s * CAP, CAP), CAP)
    ebuf[y, x, shift * CAP : (shift + 1) * CAP, :] = outgoing[own_slots, :]

    pl.semaphore_wait(barrier, ep_count - 1 + 6)

    def dispatch(group):
        def one(k):
            other, device = ep_peer(k)
            place = lax.rem(shift - k + ep_count, ep_count)
            send(
                outgoing.at[pl.ds(pl.multiple_of(other * CAP, CAP), CAP), :],
                ebuf.at[y, x, pl.ds(pl.multiple_of(place * CAP, CAP), CAP), :],
                all_send.at[group],
                all_recv.at[group],
                device,
            )

        return one

    def leg1(k):
        other, device = ep_peer(k)
        send(
            leg1_out.at[lax.div(other, 2), lax.rem(other, 2)],
            leg1_in.at[s],
            all_send.at[2],
            all_recv.at[2],
            device,
        )

    def leg2(k):
        other, device = ep_peer(k)
        send(leg2_out.at[other], leg2_in.at[s], all_send.at[3], all_recv.at[3], device)

    def deal():
        for step in range(1, 4):
            for k in range(4):
                send(
                    emit_ref.at[core_rows, near_columns(k, ring.along(0, step))],
                    emit_a.at[x, core_rows, near_place(k)],
                    all_send.at[4],
                    all_recv.at[4],
                    ring.device(0, step),
                )
            send(
                emit_ref.at[core_rows, far_columns(0, ring.along(1, step))],
                emit_b.at[y, core_rows, :],
                all_send.at[7],
                all_recv.at[7],
                ring.device(1, step),
            )

    def give_back(k):
        other, device = ep_peer(k)
        place = lax.rem(shift + k, ep_count)
        send(
            expert_out.at[pl.ds(pl.multiple_of(place * CAP, CAP), CAP), :],
            returned.at[own_slots, :],
            all_send.at[5],
            all_recv.at[5],
            device,
        )

    def all_arrived(ref, k):
        pltpu.make_async_copy(ref, ref, all_recv.at[k]).wait()

    def all_sent(ref, k):
        pltpu.make_async_copy(ref, ref, all_send.at[k]).wait()

    near_slots = outgoing.at[pl.ds(0, (near_count - 1) * CAP), :]
    far_slots = outgoing.at[pl.ds(0, near_count * CAP), :]
    others_slots = outgoing.at[pl.ds(0, slots - CAP), :]
    rows = slots // 2
    gather = [Gather(ring, ebuf, p * rows, rows, DIRECT_GATHER[p], eg_send.at[p], eg_recv.at[p]) for p in range(2)]
    scatter = [
        Scatter(
            ring,
            part,
            p * rows,
            rows,
            DIRECT_SCATTER[p],
            far.at[p],
            near.at[p],
            last.at[p],
            expert_out,
            rs_send.at[p],
            rs_recv.at[p],
        )
        for p in range(2)
    ]

    def experts_of(p):
        at = pl.ds(p * rows, rows)
        tokens = jnp.concatenate([ebuf[k // 4, k % 4, at, :] for k in range(16)], axis=1)
        opened = nt(tokens, switch_buf[...])
        opened = opened * jax.nn.sigmoid(opened)
        hidden = (opened * nt(tokens, widen_buf[...])).astype(BF16)
        for k in range(4):
            product = nn(hidden, shrink_buf[:, k * 512 : (k + 1) * 512]).astype(BF16)
            for m in range(4):
                part[k, m, at, :] = product[:, m * LANES : (m + 1) * LANES]

    for low, high in ((1, shift + 1), (ep_count - shift + 1, ep_count)):
        lax.fori_loop(low, high, lambda k, _: dispatch(0)(k), None)
    pairs(dispatch(1), near_count, near_count + 1, near_count - shift)
    deal()

    for load in loads[3:9]:
        load.wait()
    tri = iota((CHUNK, CHUNK), 0) >= iota((CHUNK, CHUNK), 1)
    tri_t = iota((CHUNK, CHUNK), 0) <= iota((CHUNK, CHUNK), 1)
    for n in range(chunks):
        at = slice(n * CHUNK, (n + 1) * CHUNK)
        query = q_ref[at, :].astype(F32)
        query = query * jax.nn.sigmoid(query)
        values = v_ref[at, :]
        spike = spikes_ref[0:1, at]
        scores = []
        for d, (pre_ref, mask, queries, added) in enumerate(
            ((right_ref, tri, query_f, added_f), (left_ref, tri_t, query_b, added_b))
        ):
            pre = pre_ref[at, :].astype(F32)
            bound = bounds_ref[d : d + 1, :]
            gap = 1.0 - bound
            log_decay = jnp.log(bound + gap * jax.nn.sigmoid(pre))
            key = gap * jax.nn.sigmoid(-pre)
            split = jnp.concatenate(three_parts(log_decay), axis=1).astype(BF16)
            summed = nn(jnp.where(mask, 1.0, 0.0).astype(BF16), split)
            total = summed[:, :LANES] + summed[:, LANES : 2 * LANES] + summed[:, 2 * LANES :]
            total = total + jnp.sum(jnp.where(mask, spike, 0.0), axis=1, keepdims=True)
            whole = total[CHUNK - 1 : CHUNK, :] if d == 0 else total[0:1, :]
            middle = total[CHUNK // 2 : CHUNK // 2 + 1, :]
            near_q = (query * jnp.exp(total - middle)).astype(BF16)
            near_k = (key * jnp.exp(middle - total)).astype(BF16)
            scores.append(jnp.where(mask, nt(near_q, near_k), 0.0))
            queries[at, :] = (query * jnp.exp(total)).astype(BF16)
            added[n] = tn(values, (key * jnp.exp(whole - total)).astype(BF16))
            chunk_decay[d, n] = whole
        intra[at, :] = nn((scores[0] + scores[1]).astype(BF16), values)

    z_count = ep_count // 2
    rows_s = LANES // z_count
    for d, (added, order) in enumerate(
        ((added_f, range(chunks)), (added_b, range(chunks - 1, -1, -1)))
    ):
        state, decay = None, None
        for n in order:
            state = added[n] if state is None else state * jnp.exp(chunk_decay[d, n]) + added[n]
            decay = chunk_decay[d, n] if decay is None else decay + chunk_decay[d, n]
        hi, mid, lo = three_parts(decay)
        row = iota((8, LANES), 0)
        tail = jnp.where(row == 0, hi, jnp.where(row == 1, mid, jnp.where(row == 2, lo, 0.0)))
        tail = jnp.broadcast_to(tail[None], (z_count, 8, LANES))
        leg1_out[:, d] = jnp.concatenate(
            [state.reshape(z_count, rows_s, LANES), tail], axis=1
        ).astype(BF16)
    leg1_in[s] = leg1_out[z, c]
    all_arrived(near_slots, 0)
    gather[0].start()
    gather[0].near()
    gather[0].far()
    loads[10].wait()
    same = iota((rows_b, rows_b), 0) == iota((rows_b, rows_b), 1)
    for k in range(2):
        taken[k] = picks[k].T
        share = jnp.sum(jnp.where(same, shares_ref[k : k + 1, :], 0.0), axis=1, keepdims=True)
        share_columns[k] = jnp.broadcast_to(share, (rows_b, LANES))
    everyone(leg1)
    gather[0].relay(0)
    all_arrived(far_slots, 1)
    gather[1].start()
    gather[0].relay(1)
    gather[0].relay(2)
    gather[0].relay(3)
    gather[1].near()
    gather[1].far()
    gather[1].relay(0)
    gather[1].relay(1)
    gather[1].relay(2)
    gather[1].relay(3)
    for load in loads[14:19]:
        load.wait()
    dealt = emit_a.at[pl.ds(0, 3), pl.ds(0, LANES // 2), :]
    all_arrived(dealt, 4)
    all_arrived(dealt, 7)
    for emit, k in ((emit_a, 6), (emit_b, 8)):
        block = emit.at[:, core_rows, :]
        send(block, block, all_send.at[k], all_recv.at[k], (z, 1 - c, y, x))
    for half in range(2):
        gather[0].finish(half)
    for load in loads[11:14]:
        load.wait()
    experts_of(0)
    for half in range(2):
        scatter[0].start(half)
    all_arrived(leg1_in.at[pl.ds(0, ep_count - 1)], 2)
    carried = jnp.zeros((rows_s, LANES), F32)
    for n in range(ep_count):
        i = jnp.where(c == 0, n, ep_count - 1 - n)
        tile = leg1_in[i].astype(F32)
        leg2_out[i] = carried.astype(BF16)
        decay = tile[rows_s : rows_s + 1] + tile[rows_s + 1 : rows_s + 2] + tile[rows_s + 2 : rows_s + 3]
        carried = carried * jnp.exp(decay) + tile[:rows_s]
    everyone(leg2)
    leg2_in[s] = leg2_out[s]
    for half in range(2):
        gather[1].finish(half)
    experts_of(1)
    for half in range(2):
        scatter[1].start(half)
    for m in range(4):
        for half in range(2):
            scatter[0].pass_on(half, m)
    for m in range(4):
        for half in range(2):
            scatter[1].pass_on(half, m)
    for m in range(4):
        for half in range(2):
            scatter[0].collect(half, m)
    for m in range(4):
        for half in range(2):
            scatter[1].collect(half, m)
    all_arrived(leg2_in.at[pl.ds(0, ep_count - 1)], 3)
    loads[9].wait()
    entries = [
        jnp.concatenate([leg2_in[2 * k + d].astype(F32) for k in range(z_count)], axis=0)
        for d in range(2)
    ]
    for d, (added, queries, order) in enumerate(
        ((added_f, query_f, range(chunks)), (added_b, query_b, range(chunks - 1, -1, -1)))
    ):
        state = entries[d]
        for n in order:
            at = slice(n * CHUNK, (n + 1) * CHUNK)
            intra[at, :] += nt(queries[at, :], state.astype(BF16))
            state = state * jnp.exp(chunk_decay[d, n]) + added[n]
    mixed = intra[...]
    mixed = mixed * lax.rsqrt(jnp.mean(mixed * mixed, axis=1, keepdims=True) + EPS)
    mixed = (mixed * gain_ref[...]).astype(BF16)
    mixed = mixed.reshape(2, 2, tok // 4, LANES)
    mixed_in[0, x] = mixed[0]
    mixed_in[1, y] = mixed[1]
    def flow_m(stage, half, part_m, step, src, dst, axis):
        return pltpu.make_async_remote_copy(
            src_ref=src,
            dst_ref=dst,
            send_sem=m_send.at[stage, half, part_m, step],
            recv_sem=m_recv.at[stage, half, part_m, step],
            device_id=ring.device(axis, step),
            device_id_type=MESH,
        )

    flows_m = []
    for part_m in range(2):
        for half in range(2):
            own = mixed_in.at[half, (x, y)[half], part_m]
            for step in range(1, 4):
                flows_m.append(flow_m(0, half, part_m, step, own, own, half))

    def heads_out(core):
        @pl.when(c == core)
        def _():
            for flow in flows_m[:12]:
                flow.start()

    heads_out(0)
    for half in range(2):
        scatter[0].end(half)
    pairs(give_back, shift - 1, ep_count - shift, shift - 1)
    give_back(ep_count - 1)
    returned[own_slots, :] = expert_out[shift * CAP : (shift + 1) * CAP, :]
    for half in range(2):
        scatter[1].end(half)
    give_back(near_count)
    pairs(give_back, near_count - 1, near_count + 1, near_count - shift - 1)
    give_back(shift)
    heads_out(1)
    whole = emit_a.at[:, pl.ds(0, LANES // 2), :]
    all_arrived(whole, 6)
    all_arrived(whole, 8)

    def heads_in(part_m):
        for half in range(2):
            for step in range(1, 4):
                come = mixed_in.at[half, ring.along(half, step), part_m]
                pltpu.make_async_copy(come, come, m_recv.at[0, half, part_m, step]).wait()
            heads = jnp.concatenate([mixed_in[half, k, part_m] for k in range(4)], axis=1)
            emit = (emit_a, emit_b)[half][...].reshape(4 * LANES, 4 * LANES)
            product = nn(heads, emit)
            for k in range(4):
                mixed_part[half, k, part_m] = product[:, k * LANES : (k + 1) * LANES].astype(BF16)
            for step in range(1, 4):
                flow = flow_m(
                    1,
                    half,
                    part_m,
                    step,
                    mixed_part.at[half, ring.along(1 - half, step), part_m],
                    mixed_come.at[half, step, part_m],
                    1 - half,
                )
                flow.start()
                flows_m.append(flow)

    heads_in(0)
    heads_in(1)
    for part_m in range(2):
        for half in range(2):
            total = mixed_part[half, (y, x)[half], part_m].astype(F32)
            for step in range(1, 4):
                come = mixed_come.at[half, step, part_m]
                pltpu.make_async_copy(come, come, m_recv.at[1, half, part_m, step]).wait()
                total = total + mixed_come[half, step, part_m].astype(F32)
            start = (2 * half + part_m) * (tok // 4)
            out_a_ref[start : start + tok // 4, :] = total.astype(BF16)
    all_sent(near_slots, 0)
    all_sent(far_slots, 1)
    all_sent(leg1_in.at[pl.ds(0, ep_count - 1)], 2)
    all_sent(leg2_in.at[pl.ds(0, ep_count - 1)], 3)
    for k in (4, 7):
        all_sent(dealt, k)
    for k in (6, 8):
        all_sent(whole, k)
    for copy in flows_m:
        copy.wait_send()
    for flow in (*gather, *scatter):
        flow.drain()
    all_arrived(others_slots, 5)
    all_sent(others_slots, 5)
    results = returned[...]
    mixed_b = jnp.zeros((rows_b, LANES), F32)
    for k in range(2):
        mixed_b = mixed_b + nn(taken[k], results) * share_columns[k]
    out_b_ref[...] = mixed_b.astype(BF16)


def per_device(*args):
    (q, right, left, v, bounds, spikes, gain, emit, rows, rows_gain, ids, shares, switch, widen, shrink) = args
    ep_count = lax.axis_size("z") * 2
    tok, rows_b, width = q.shape[0], rows.shape[0], rows.shape[1]
    hidden = switch.shape[2]
    slots = ep_count * CAP
    chunks = tok // CHUNK
    z_count = ep_count // 2
    rows_s = LANES // z_count
    n = slots // 4
    dma = pltpu.SemaphoreType.DMA
    return pl.pallas_call(
        functools.partial(kernel, ep_count),
        out_shape=(
            pltpu.VMEM((tok, LANES), BF16),
            pltpu.VMEM((rows_b, LANES), BF16),
        ),
        in_specs=[pl.BlockSpec(memory_space=pl.ANY)] * 15,
        out_specs=(pl.BlockSpec(memory_space=pltpu.VMEM),) * 2,
        scratch_shapes=[
            pltpu.VMEM((tok, LANES), BF16),
            pltpu.VMEM((tok, LANES), BF16),
            pltpu.VMEM((tok, LANES), BF16),
            pltpu.VMEM((tok, LANES), BF16),
            pltpu.VMEM((2, LANES), F32),
            pltpu.VMEM((1, tok), F32),
            pltpu.VMEM((1, LANES), F32),
            pltpu.VMEM((rows_b, width), BF16),
            pltpu.VMEM((1, width), F32),
            pltpu.VMEM((2, rows_b), jnp.int32),
            pltpu.VMEM((2, rows_b), F32),
            pltpu.VMEM((hidden, width), BF16),
            pltpu.VMEM((hidden, width), BF16),
            pltpu.VMEM((hidden, width), BF16),
            pltpu.VMEM((4, LANES, 4 * LANES), BF16),
            pltpu.VMEM((4, LANES, 4 * LANES), BF16),
            pltpu.VMEM((slots, LANES), BF16),
            pltpu.VMEM((4, 4, slots, LANES), BF16),
            pltpu.VMEM((4, 4, slots, LANES), BF16),
            pltpu.VMEM((2, 2, 4, n, LANES), BF16),
            pltpu.VMEM((2, 2, 2, 4, n, LANES), BF16),
            pltpu.VMEM((2, 2, 3, n, LANES), BF16),
            pltpu.VMEM((slots, LANES), BF16),
            pltpu.VMEM((slots, LANES), BF16),
            pltpu.VMEM((2, slots, rows_b), BF16),
            pltpu.VMEM((2, rows_b, slots), BF16),
            pltpu.VMEM((2, rows_b, LANES), F32),
            pltpu.VMEM((tok, LANES), F32),
            pltpu.VMEM((tok, LANES), BF16),
            pltpu.VMEM((tok, LANES), BF16),
            pltpu.VMEM((chunks, LANES, LANES), F32),
            pltpu.VMEM((chunks, LANES, LANES), F32),
            pltpu.VMEM((2, chunks, 1, LANES), F32),
            pltpu.VMEM((z_count, 2, rows_s + 8, LANES), BF16),
            pltpu.VMEM((ep_count, rows_s + 8, LANES), BF16),
            pltpu.VMEM((ep_count, rows_s, LANES), BF16),
            pltpu.VMEM((ep_count, rows_s, LANES), BF16),
            pltpu.VMEM((2, 4, 2, tok // 4, LANES), BF16),
            pltpu.VMEM((2, 4, 2, tok // 4, LANES), BF16),
            pltpu.VMEM((2, 4, 2, tok // 4, LANES), BF16),
            dma((19,)),
            dma((9,)),
            dma((9,)),
            dma((2, 2, 20)),
            dma((2, 2, 20)),
            dma((2, 2, 2, 4)),
            dma((2, 2, 2, 4)),
            dma((2, 2, 20)),
            dma((2, 2, 20)),
        ],
        compiler_params=pltpu.CompilerParams(collective_id=0, has_side_effects=True),
    )(
        q,
        right,
        left,
        v,
        bounds,
        spikes,
        gain.reshape(1, -1),
        emit,
        rows,
        rows_gain.reshape(1, -1),
        ids.T,
        shares.T,
        switch.transpose(0, 2, 1),
        widen.transpose(0, 2, 1),
        shrink,
    )


def solution(mesh):
    ep, tp = mesh.shape["ep"], mesh.shape["tp"]
    split = Mesh(mesh.devices.reshape(ep // 2, 2, tp // 4, 4), ("z", "c", "y", "x"))
    e, f = ("z", "c"), ("y", "x")
    return jax.shard_map(
        per_device,
        mesh=split,
        in_specs=(
            P(e, f),
            P(e, f),
            P(e, f),
            P(e, f),
            P(None, f),
            P(f, e),
            P(f),
            P(f, None),
            P(e, None),
            P(),
            P(e, None),
            P(e, None),
            P(e, None, f),
            P(e, None, f),
            P(e, f, None),
        ),
        out_specs=(P(e, f), P(e, f)),
        check_vma=False,
    )
```

```python
import functools

import jax
import jax.numpy as jnp
from jax import lax
from jax.experimental import pallas as pl
from jax.experimental.pallas import tpu as pltpu
from jax.sharding import Mesh
from jax.sharding import PartitionSpec as P

EPS = 1e-06
CAP = 16
LANES = 128
CHUNK = 128
DIRECT_GATHER = (False, True)
DIRECT_SCATTER = (False, False)
MESH = pl.DeviceIdType.MESH
F32 = jnp.float32
BF16 = jnp.bfloat16


def nn(a, b):
    return lax.dot_general(a, b, (((1,), (0,)), ((), ())), preferred_element_type=F32)


def nt(a, b):
    return lax.dot_general(a, b, (((1,), (1,)), ((), ())), preferred_element_type=F32)


def tn(a, b):
    return lax.dot_general(a, b, (((0,), (0,)), ((), ())), preferred_element_type=F32)


def iota(shape, dim):
    return lax.broadcasted_iota(jnp.int32, shape, dim)


def three_parts(a):
    hi = a.astype(BF16).astype(F32)
    rest = a - hi
    mid = rest.astype(BF16).astype(F32)
    return hi, mid, (rest - mid).astype(BF16).astype(F32)


def send(src, dst, send_sem, recv_sem, device):
    copy = pltpu.make_async_remote_copy(
        src_ref=src,
        dst_ref=dst,
        send_sem=send_sem,
        recv_sem=recv_sem,
        device_id=device,
        device_id_type=MESH,
    )
    copy.start()
    return copy


class Ring:
    def __init__(self, z, c, y, x):
        self.z, self.c, self.y, self.x = z, c, y, x

    def along(self, axis, step):
        return lax.rem((self.x if axis == 0 else self.y) + step, 4)

    def device(self, axis, step):
        there = self.along(axis, step)
        return (self.z, self.c, self.y, there) if axis == 0 else (self.z, self.c, there, self.x)


class Gather:
    ORDER = (0, 3, 1, 2)

    def __init__(self, ring, buf, base, rows, direct, send_sems, recv_sems):
        self.ring, self.buf, self.base, self.rows, self.direct = ring, buf, base, rows, direct
        self.send_sems, self.recv_sems = send_sems, recv_sems
        self.sent = []

    def block(self, half, first, second, part):
        a, b = self.ring.along(half, first), self.ring.along(1 - half, second)
        y, x = (b, a) if half == 0 else (a, b)
        n = self.rows // 2
        start, size = {None: (0, n), 0: (0, n // 2), 1: (n // 2, n // 2)}[part]
        return self.buf.at[y, x, pl.ds(self.base + half * n + start, size), :]

    def go(self, half, axis, step, block, k):
        self.sent.append(
            send(
                block,
                block,
                self.send_sems.at[half, k],
                self.recv_sems.at[half, k],
                self.ring.device(axis, step),
            )
        )

    def arrived(self, half, block, k):
        pltpu.make_async_copy(block, block, self.recv_sems.at[half, k]).wait()

    def second(self, half, n):
        first = self.ORDER[n]
        block = self.block(half, first, 0, None)
        self.go(half, 1 - half, 1, block, 4 + 4 * n)
        self.go(half, 1 - half, 3, block, 5 + 4 * n)
        if self.direct:
            self.go(half, 1 - half, 2, block, 6 + 4 * n)

    def start(self):
        for half in range(2):
            block = self.block(half, 0, 0, None)
            self.go(half, half, 1, block, 0)
            self.go(half, half, 3, block, 1)
            self.go(half, half, 2, block, 2)
        for half in range(2):
            self.second(half, 0)

    def near(self):
        for half in range(2):
            self.arrived(half, self.block(half, 3, 0, None), 0)
            self.second(half, 1)
            self.arrived(half, self.block(half, 1, 0, None), 1)
            self.second(half, 2)

    def far(self):
        for half in range(2):
            self.arrived(half, self.block(half, 2, 0, None), 2)
            self.second(half, 3)

    def relay(self, n):
        first = self.ORDER[n]
        for half in () if self.direct else range(2):
            self.arrived(half, self.block(half, first, 3, None), 4 + 4 * n)
            self.go(half, 1 - half, 1, self.block(half, first, 3, 0), 6 + 4 * n)
            self.arrived(half, self.block(half, first, 1, None), 5 + 4 * n)
            self.go(half, 1 - half, 3, self.block(half, first, 1, 1), 7 + 4 * n)

    def finish(self, half):
        for n in range(4):
            first = self.ORDER[n]
            if self.direct:
                self.arrived(half, self.block(half, first, 3, None), 4 + 4 * n)
                self.arrived(half, self.block(half, first, 1, None), 5 + 4 * n)
                self.arrived(half, self.block(half, first, 2, None), 6 + 4 * n)
            else:
                self.arrived(half, self.block(half, first, 2, 0), 6 + 4 * n)
                self.arrived(half, self.block(half, first, 2, 1), 7 + 4 * n)

    def drain(self):
        for copy in self.sent:
            copy.wait_send()


class Scatter:
    ORDER = (2, 1, 3, 0)

    def __init__(self, ring, part, base, rows, direct, far, near, last, out, send_sems, recv_sems):
        self.ring, self.part, self.base, self.direct, self.out = ring, part, base, direct, out
        self.far, self.near, self.last = far, near, last
        self.send_sems, self.recv_sems = send_sems, recv_sems
        self.n = rows // 2
        self.sent = []

    def block(self, half, first, second, lo, size):
        axis = 1 - half
        a, b = self.ring.along(axis, first), self.ring.along(1 - axis, second)
        y, x = (a, b) if axis == 1 else (b, a)
        return self.part.at[y, x, pl.ds(self.base + half * self.n + lo, size), :]

    def go(self, half, axis, step, src, dst, k):
        self.sent.append(
            send(
                src,
                dst,
                self.send_sems.at[half, k],
                self.recv_sems.at[half, k],
                self.ring.device(axis, step),
            )
        )

    def arrived(self, half, ref, k):
        pltpu.make_async_copy(ref, ref, self.recv_sems.at[half, k]).wait()

    def start(self, half):
        q = self.n // 2
        for m in range(4):
            o = self.ORDER[m]
            if self.direct:
                for way, step in ((0, 1), (1, 3)):
                    src = self.block(half, step, o, 0, self.n)
                    self.go(half, 1 - half, step, src, self.near.at[half, way, m], 4 * m + 2 + way)
                src = self.block(half, 2, o, 0, self.n)
                self.go(half, 1 - half, 2, src, self.far.at[half, m], 4 * m)
            else:
                for way, step in ((0, 1), (1, 3)):
                    src = self.block(half, 2, o, way * q, q)
                    dst = self.far.at[half, m, pl.ds(way * q, q), :]
                    self.go(half, 1 - half, step, src, dst, 4 * m + way)

    def pass_on(self, half, m):
        q, o = self.n // 2, self.ORDER[m]
        for way, step in () if self.direct else ((0, 1), (1, 3)):
            come = self.far.at[half, m, pl.ds(way * q, q), :]
            self.arrived(half, come, 4 * m + way)
            mine = self.block(half, step, o, way * q, q)
            mine[...] = (mine[...].astype(F32) + come[...].astype(F32)).astype(BF16)
            self.go(
                half,
                1 - half,
                step,
                self.block(half, step, o, 0, self.n),
                self.near.at[half, way, m],
                4 * m + 2 + way,
            )

    def collect(self, half, m):
        o = self.ORDER[m]
        for way in range(2):
            self.arrived(half, self.near.at[half, way, m], 4 * m + 2 + way)
        mine = self.block(half, 0, o, 0, self.n)
        total = mine[...].astype(F32) + self.near[half, 0, m].astype(F32)
        total = total + self.near[half, 1, m].astype(F32)
        if self.direct:
            self.arrived(half, self.far.at[half, m], 4 * m)
            total = total + self.far[half, m].astype(F32)
        mine[...] = total.astype(BF16)
        if m < 3:
            self.go(half, half, o, mine, self.last.at[half, m], 16 + m)

    def end(self, half):
        total = self.block(half, 0, 0, 0, self.n)[...].astype(F32)
        for m in (1, 2, 0):
            self.arrived(half, self.last.at[half, m], 16 + m)
            total = total + self.last[half, m].astype(F32)
        self.out[pl.ds(self.base + half * self.n, self.n), :] = total.astype(BF16)

    def drain(self):
        for copy in self.sent:
            copy.wait_send()


def kernel(
    ep_count,
    q_hbm,
    right_hbm,
    left_hbm,
    v_hbm,
    bounds_hbm,
    spikes_hbm,
    gain_hbm,
    emit_ref,
    rows_hbm,
    rows_gain_hbm,
    ids_hbm,
    shares_hbm,
    switch_ref,
    widen_ref,
    shrink_ref,
    out_a_ref,
    out_b_ref,
    q_ref,
    right_ref,
    left_ref,
    v_ref,
    bounds_ref,
    spikes_ref,
    gain_ref,
    rows_ref,
    rows_gain_ref,
    ids_ref,
    shares_ref,
    switch_buf,
    widen_buf,
    shrink_buf,
    emit_a,
    emit_b,
    outgoing,
    ebuf,
    part,
    far,
    near,
    last,
    expert_out,
    returned,
    picks,
    taken,
    share_columns,
    intra,
    query_f,
    query_b,
    added_f,
    added_b,
    chunk_decay,
    leg1_out,
    leg1_in,
    leg2_out,
    leg2_in,
    mixed_in,
    mixed_part,
    mixed_come,
    load_sems,
    all_send,
    all_recv,
    eg_send,
    eg_recv,
    m_send,
    m_recv,
    rs_send,
    rs_recv,
):
    z, c = lax.axis_index("z"), lax.axis_index("c")
    y, x = lax.axis_index("y"), lax.axis_index("x")
    s, t = 2 * z + c, 4 * y + x
    ring = Ring(z, c, y, x)
    tok = q_ref.shape[0]
    chunks = tok // CHUNK
    rows_b = rows_ref.shape[0]
    slots = ep_count * CAP
    near_count = ep_count // 2
    shift = ep_count // 4

    def ep_peer(k):
        other = lax.rem(s + k, ep_count)
        return other, (lax.div(other, 2), lax.rem(other, 2), y, x)

    columns = pl.ds(pl.multiple_of(t * LANES, LANES), LANES)

    def far_columns(_, to):
        return pl.ds(pl.multiple_of(to * (4 * LANES), 4 * LANES), 4 * LANES)

    def near_columns(k, to):
        return pl.ds(pl.multiple_of((4 * k + to) * LANES, LANES), LANES)

    def near_place(k):
        return pl.ds(k * LANES, LANES)

    core_rows = pl.ds(pl.multiple_of(c * (LANES // 2), LANES // 2), LANES // 2)
    loads = [
        pltpu.make_async_copy(src, dst, load_sems.at[i])
        for i, (src, dst) in enumerate(
            (
                (ids_hbm, ids_ref),
                (rows_hbm, rows_ref),
                (rows_gain_hbm, rows_gain_ref),
                (bounds_hbm, bounds_ref),
                (spikes_hbm, spikes_ref),
                (q_hbm, q_ref),
                (right_hbm, right_ref),
                (left_hbm, left_ref),
                (v_hbm, v_ref),
                (gain_hbm, gain_ref),
                (shares_hbm, shares_ref),
                (switch_ref.at[0], switch_buf),
                (widen_ref.at[0], widen_buf),
                (shrink_ref.at[0], shrink_buf),
                (emit_ref.at[core_rows, far_columns(0, y)], emit_b.at[y, core_rows, :]),
                *(
                    (emit_ref.at[core_rows, near_columns(k, x)], emit_a.at[x, core_rows, near_place(k)])
                    for k in range(4)
                ),
            )
        )
    ]
    for load in loads:
        load.start()
    barrier = pltpu.get_barrier_semaphore()

    def greet(k):
        pl.semaphore_signal(barrier, inc=1, device_id=ep_peer(k)[1], device_id_type=MESH)

    def pairs(one, low, high, count):
        def both(i, _):
            one(low - i)
            one(high + i)
            return _

        lax.fori_loop(0, count, both, 0)

    def everyone(one):
        one(near_count)
        pairs(one, near_count - 1, near_count + 1, near_count - 1)

    everyone(greet)
    for axis in range(2):
        for step in range(1, 4):
            pl.semaphore_signal(
                barrier, inc=1, device_id=ring.device(axis, step), device_id_type=MESH
            )

    for load in loads[:3]:
        load.wait()

    width = rows_ref.shape[1]
    square = jnp.zeros((rows_b, LANES), F32)
    for k in range(width // LANES):
        piece = rows_ref[:, k * LANES : (k + 1) * LANES].astype(F32)
        square = square + piece * piece
    mean = jnp.sum(square, axis=1, keepdims=True) / width
    normed = rows_ref[:, columns].astype(F32) * lax.rsqrt(mean + EPS)
    normed = (normed * rows_gain_ref[:, columns]).astype(BF16)
    experts = iota((ep_count, rows_b), 0)
    pick0 = ids_ref[0:1, :] == experts
    pick1 = ids_ref[1:2, :] == experts
    named = (pick0 | pick1).astype(F32).astype(BF16)
    earlier = (iota((rows_b, rows_b), 0) < iota((rows_b, rows_b), 1)).astype(F32).astype(BF16)
    rank = nn(named, earlier)
    at_slot = rank.astype(jnp.int32)[:, None, :] == iota((ep_count, CAP, rows_b), 1)
    ones = jnp.where(at_slot, 1.0, 0.0)
    for k, pick in enumerate((pick0, pick1)):
        chosen = ones * jnp.where(pick, 1.0, 0.0)[:, None, :]
        picks[k] = chosen.reshape(slots, rows_b).astype(BF16)
    outgoing[...] = nn(picks[0] + picks[1], normed).astype(BF16)
    own_slots = pl.ds(pl.multiple_of(s * CAP, CAP), CAP)
    ebuf[y, x, shift * CAP : (shift + 1) * CAP, :] = outgoing[own_slots, :]

    pl.semaphore_wait(barrier, ep_count - 1 + 6)

    def dispatch(group):
        def one(k):
            other, device = ep_peer(k)
            place = lax.rem(shift - k + ep_count, ep_count)
            send(
                outgoing.at[pl.ds(pl.multiple_of(other * CAP, CAP), CAP), :],
                ebuf.at[y, x, pl.ds(pl.multiple_of(place * CAP, CAP), CAP), :],
                all_send.at[group],
                all_recv.at[group],
                device,
            )

        return one

    def leg1(k):
        other, device = ep_peer(k)
        send(
            leg1_out.at[lax.div(other, 2), lax.rem(other, 2)],
            leg1_in.at[s],
            all_send.at[2],
            all_recv.at[2],
            device,
        )

    def leg2(k):
        other, device = ep_peer(k)
        send(leg2_out.at[other], leg2_in.at[s], all_send.at[3], all_recv.at[3], device)

    def deal():
        for step in range(1, 4):
            for k in range(4):
                send(
                    emit_ref.at[core_rows, near_columns(k, ring.along(0, step))],
                    emit_a.at[x, core_rows, near_place(k)],
                    all_send.at[4],
                    all_recv.at[4],
                    ring.device(0, step),
                )
            send(
                emit_ref.at[core_rows, far_columns(0, ring.along(1, step))],
                emit_b.at[y, core_rows, :],
                all_send.at[7],
                all_recv.at[7],
                ring.device(1, step),
            )

    def give_back(k):
        other, device = ep_peer(k)
        place = lax.rem(shift + k, ep_count)
        send(
            expert_out.at[pl.ds(pl.multiple_of(place * CAP, CAP), CAP), :],
            returned.at[own_slots, :],
            all_send.at[5],
            all_recv.at[5],
            device,
        )

    def all_arrived(ref, k):
        pltpu.make_async_copy(ref, ref, all_recv.at[k]).wait()

    def all_sent(ref, k):
        pltpu.make_async_copy(ref, ref, all_send.at[k]).wait()

    near_slots = outgoing.at[pl.ds(0, (near_count - 1) * CAP), :]
    far_slots = outgoing.at[pl.ds(0, near_count * CAP), :]
    others_slots = outgoing.at[pl.ds(0, slots - CAP), :]
    rows = slots // 2
    gather = [Gather(ring, ebuf, p * rows, rows, DIRECT_GATHER[p], eg_send.at[p], eg_recv.at[p]) for p in range(2)]
    scatter = [
        Scatter(
            ring,
            part,
            p * rows,
            rows,
            DIRECT_SCATTER[p],
            far.at[p],
            near.at[p],
            last.at[p],
            expert_out,
            rs_send.at[p],
            rs_recv.at[p],
        )
        for p in range(2)
    ]

    def experts_of(p):
        at = pl.ds(p * rows, rows)
        tokens = jnp.concatenate([ebuf[k // 4, k % 4, at, :] for k in range(16)], axis=1)
        opened = nt(tokens, switch_buf[...])
        opened = opened * jax.nn.sigmoid(opened)
        hidden = (opened * nt(tokens, widen_buf[...])).astype(BF16)
        for k in range(4):
            product = nn(hidden, shrink_buf[:, k * 512 : (k + 1) * 512]).astype(BF16)
            for m in range(4):
                part[k, m, at, :] = product[:, m * LANES : (m + 1) * LANES]

    for low, high in ((1, shift + 1), (ep_count - shift + 1, ep_count)):
        lax.fori_loop(low, high, lambda k, _: dispatch(0)(k), None)
    pairs(dispatch(1), near_count, near_count + 1, near_count - shift)
    deal()

    for load in loads[3:9]:
        load.wait()
    tri = iota((CHUNK, CHUNK), 0) >= iota((CHUNK, CHUNK), 1)
    tri_t = iota((CHUNK, CHUNK), 0) <= iota((CHUNK, CHUNK), 1)
    for n in range(chunks):
        at = slice(n * CHUNK, (n + 1) * CHUNK)
        query = q_ref[at, :].astype(F32)
        query = query * jax.nn.sigmoid(query)
        values = v_ref[at, :]
        spike = spikes_ref[0:1, at]
        scores = []
        for d, (pre_ref, mask, queries, added) in enumerate(
            ((right_ref, tri, query_f, added_f), (left_ref, tri_t, query_b, added_b))
        ):
            pre = pre_ref[at, :].astype(F32)
            bound = bounds_ref[d : d + 1, :]
            gap = 1.0 - bound
            log_decay = jnp.log(bound + gap * jax.nn.sigmoid(pre))
            key = gap * jax.nn.sigmoid(-pre)
            split = jnp.concatenate(three_parts(log_decay), axis=1).astype(BF16)
            summed = nn(jnp.where(mask, 1.0, 0.0).astype(BF16), split)
            total = summed[:, :LANES] + summed[:, LANES : 2 * LANES] + summed[:, 2 * LANES :]
            total = total + jnp.sum(jnp.where(mask, spike, 0.0), axis=1, keepdims=True)
            whole = total[CHUNK - 1 : CHUNK, :] if d == 0 else total[0:1, :]
            middle = total[CHUNK // 2 : CHUNK // 2 + 1, :]
            near_q = (query * jnp.exp(total - middle)).astype(BF16)
            near_k = (key * jnp.exp(middle - total)).astype(BF16)
            scores.append(jnp.where(mask, nt(near_q, near_k), 0.0))
            queries[at, :] = (query * jnp.exp(total)).astype(BF16)
            added[n] = tn(values, (key * jnp.exp(whole - total)).astype(BF16))
            chunk_decay[d, n] = whole
        intra[at, :] = nn((scores[0] + scores[1]).astype(BF16), values)

    z_count = ep_count // 2
    rows_s = LANES // z_count
    for d, (added, order) in enumerate(
        ((added_f, range(chunks)), (added_b, range(chunks - 1, -1, -1)))
    ):
        state, decay = None, None
        for n in order:
            state = added[n] if state is None else state * jnp.exp(chunk_decay[d, n]) + added[n]
            decay = chunk_decay[d, n] if decay is None else decay + chunk_decay[d, n]
        hi, mid, lo = three_parts(decay)
        row = iota((8, LANES), 0)
        tail = jnp.where(row == 0, hi, jnp.where(row == 1, mid, jnp.where(row == 2, lo, 0.0)))
        tail = jnp.broadcast_to(tail[None], (z_count, 8, LANES))
        leg1_out[:, d] = jnp.concatenate(
            [state.reshape(z_count, rows_s, LANES), tail], axis=1
        ).astype(BF16)
    leg1_in[s] = leg1_out[z, c]
    all_arrived(near_slots, 0)
    gather[0].start()
    gather[0].near()
    gather[0].far()
    loads[10].wait()
    same = iota((rows_b, rows_b), 0) == iota((rows_b, rows_b), 1)
    for k in range(2):
        taken[k] = picks[k].T
        share = jnp.sum(jnp.where(same, shares_ref[k : k + 1, :], 0.0), axis=1, keepdims=True)
        share_columns[k] = jnp.broadcast_to(share, (rows_b, LANES))
    everyone(leg1)
    gather[0].relay(0)
    all_arrived(far_slots, 1)
    gather[1].start()
    gather[0].relay(1)
    gather[0].relay(2)
    gather[0].relay(3)
    gather[1].near()
    gather[1].far()
    gather[1].relay(0)
    gather[1].relay(1)
    gather[1].relay(2)
    gather[1].relay(3)
    for load in loads[14:19]:
        load.wait()
    dealt = emit_a.at[pl.ds(0, 3), pl.ds(0, LANES // 2), :]
    all_arrived(dealt, 4)
    all_arrived(dealt, 7)
    for emit, k in ((emit_a, 6), (emit_b, 8)):
        block = emit.at[:, core_rows, :]
        send(block, block, all_send.at[k], all_recv.at[k], (z, 1 - c, y, x))
    for half in range(2):
        gather[0].finish(half)
    for load in loads[11:14]:
        load.wait()
    experts_of(0)
    for half in range(2):
        scatter[0].start(half)
    all_arrived(leg1_in.at[pl.ds(0, ep_count - 1)], 2)
    carried = jnp.zeros((rows_s, LANES), F32)
    for n in range(ep_count):
        i = jnp.where(c == 0, n, ep_count - 1 - n)
        tile = leg1_in[i].astype(F32)
        leg2_out[i] = carried.astype(BF16)
        decay = tile[rows_s : rows_s + 1] + tile[rows_s + 1 : rows_s + 2] + tile[rows_s + 2 : rows_s + 3]
        carried = carried * jnp.exp(decay) + tile[:rows_s]
    everyone(leg2)
    leg2_in[s] = leg2_out[s]
    for half in range(2):
        gather[1].finish(half)
    experts_of(1)
    for half in range(2):
        scatter[1].start(half)
    for m in range(4):
        for half in range(2):
            scatter[1].pass_on(half, m)
    for m in range(4):
        for half in range(2):
            scatter[0].pass_on(half, m)
    for m in range(4):
        for half in range(2):
            scatter[1].collect(half, m)
    for m in range(4):
        for half in range(2):
            scatter[0].collect(half, m)
    all_arrived(leg2_in.at[pl.ds(0, ep_count - 1)], 3)
    loads[9].wait()
    entries = [
        jnp.concatenate([leg2_in[2 * k + d].astype(F32) for k in range(z_count)], axis=0)
        for d in range(2)
    ]
    for d, (added, queries, order) in enumerate(
        ((added_f, query_f, range(chunks)), (added_b, query_b, range(chunks - 1, -1, -1)))
    ):
        state = entries[d]
        for n in order:
            at = slice(n * CHUNK, (n + 1) * CHUNK)
            intra[at, :] += nt(queries[at, :], state.astype(BF16))
            state = state * jnp.exp(chunk_decay[d, n]) + added[n]
    mixed = intra[...]
    mixed = mixed * lax.rsqrt(jnp.mean(mixed * mixed, axis=1, keepdims=True) + EPS)
    mixed = (mixed * gain_ref[...]).astype(BF16)
    mixed = mixed.reshape(2, 2, tok // 4, LANES)
    mixed_in[0, x] = mixed[0]
    mixed_in[1, y] = mixed[1]
    def flow_m(stage, half, part_m, step, src, dst, axis):
        return pltpu.make_async_remote_copy(
            src_ref=src,
            dst_ref=dst,
            send_sem=m_send.at[stage, half, part_m, step],
            recv_sem=m_recv.at[stage, half, part_m, step],
            device_id=ring.device(axis, step),
            device_id_type=MESH,
        )

    flows_m = []
    for part_m in range(2):
        for half in range(2):
            own = mixed_in.at[half, (x, y)[half], part_m]
            for step in range(1, 4):
                flows_m.append(flow_m(0, half, part_m, step, own, own, half))

    def heads_out(core):
        @pl.when(c == core)
        def _():
            for flow in flows_m[:12]:
                flow.start()

    heads_out(0)
    for half in range(2):
        scatter[1].end(half)
    give_back(near_count)
    pairs(give_back, near_count - 1, near_count + 1, near_count - shift - 1)
    give_back(shift)
    for half in range(2):
        scatter[0].end(half)
    pairs(give_back, shift - 1, ep_count - shift, shift - 1)
    give_back(ep_count - 1)
    returned[own_slots, :] = expert_out[shift * CAP : (shift + 1) * CAP, :]
    heads_out(1)
    whole = emit_a.at[:, pl.ds(0, LANES // 2), :]
    all_arrived(whole, 6)
    all_arrived(whole, 8)

    def heads_in(part_m):
        for half in range(2):
            for step in range(1, 4):
                come = mixed_in.at[half, ring.along(half, step), part_m]
                pltpu.make_async_copy(come, come, m_recv.at[0, half, part_m, step]).wait()
            heads = jnp.concatenate([mixed_in[half, k, part_m] for k in range(4)], axis=1)
            emit = (emit_a, emit_b)[half][...].reshape(4 * LANES, 4 * LANES)
            product = nn(heads, emit)
            for k in range(4):
                mixed_part[half, k, part_m] = product[:, k * LANES : (k + 1) * LANES].astype(BF16)
            for step in range(1, 4):
                flow = flow_m(
                    1,
                    half,
                    part_m,
                    step,
                    mixed_part.at[half, ring.along(1 - half, step), part_m],
                    mixed_come.at[half, step, part_m],
                    1 - half,
                )
                flow.start()
                flows_m.append(flow)

    heads_in(0)
    heads_in(1)
    for part_m in range(2):
        for half in range(2):
            total = mixed_part[half, (y, x)[half], part_m].astype(F32)
            for step in range(1, 4):
                come = mixed_come.at[half, step, part_m]
                pltpu.make_async_copy(come, come, m_recv.at[1, half, part_m, step]).wait()
                total = total + mixed_come[half, step, part_m].astype(F32)
            start = (2 * half + part_m) * (tok // 4)
            out_a_ref[start : start + tok // 4, :] = total.astype(BF16)
    all_sent(near_slots, 0)
    all_sent(far_slots, 1)
    all_sent(leg1_in.at[pl.ds(0, ep_count - 1)], 2)
    all_sent(leg2_in.at[pl.ds(0, ep_count - 1)], 3)
    for k in (4, 7):
        all_sent(dealt, k)
    for k in (6, 8):
        all_sent(whole, k)
    for copy in flows_m:
        copy.wait_send()
    for flow in (*gather, *scatter):
        flow.drain()
    all_arrived(others_slots, 5)
    all_sent(others_slots, 5)
    results = returned[...]
    mixed_b = jnp.zeros((rows_b, LANES), F32)
    for k in range(2):
        mixed_b = mixed_b + nn(taken[k], results) * share_columns[k]
    out_b_ref[...] = mixed_b.astype(BF16)


def per_device(*args):
    (q, right, left, v, bounds, spikes, gain, emit, rows, rows_gain, ids, shares, switch, widen, shrink) = args
    ep_count = lax.axis_size("z") * 2
    tok, rows_b, width = q.shape[0], rows.shape[0], rows.shape[1]
    hidden = switch.shape[2]
    slots = ep_count * CAP
    chunks = tok // CHUNK
    z_count = ep_count // 2
    rows_s = LANES // z_count
    n = slots // 4
    dma = pltpu.SemaphoreType.DMA
    return pl.pallas_call(
        functools.partial(kernel, ep_count),
        out_shape=(
            pltpu.VMEM((tok, LANES), BF16),
            pltpu.VMEM((rows_b, LANES), BF16),
        ),
        in_specs=[pl.BlockSpec(memory_space=pl.ANY)] * 15,
        out_specs=(pl.BlockSpec(memory_space=pltpu.VMEM),) * 2,
        scratch_shapes=[
            pltpu.VMEM((tok, LANES), BF16),
            pltpu.VMEM((tok, LANES), BF16),
            pltpu.VMEM((tok, LANES), BF16),
            pltpu.VMEM((tok, LANES), BF16),
            pltpu.VMEM((2, LANES), F32),
            pltpu.VMEM((1, tok), F32),
            pltpu.VMEM((1, LANES), F32),
            pltpu.VMEM((rows_b, width), BF16),
            pltpu.VMEM((1, width), F32),
            pltpu.VMEM((2, rows_b), jnp.int32),
            pltpu.VMEM((2, rows_b), F32),
            pltpu.VMEM((hidden, width), BF16),
            pltpu.VMEM((hidden, width), BF16),
            pltpu.VMEM((hidden, width), BF16),
            pltpu.VMEM((4, LANES, 4 * LANES), BF16),
            pltpu.VMEM((4, LANES, 4 * LANES), BF16),
            pltpu.VMEM((slots, LANES), BF16),
            pltpu.VMEM((4, 4, slots, LANES), BF16),
            pltpu.VMEM((4, 4, slots, LANES), BF16),
            pltpu.VMEM((2, 2, 4, n, LANES), BF16),
            pltpu.VMEM((2, 2, 2, 4, n, LANES), BF16),
            pltpu.VMEM((2, 2, 3, n, LANES), BF16),
            pltpu.VMEM((slots, LANES), BF16),
            pltpu.VMEM((slots, LANES), BF16),
            pltpu.VMEM((2, slots, rows_b), BF16),
            pltpu.VMEM((2, rows_b, slots), BF16),
            pltpu.VMEM((2, rows_b, LANES), F32),
            pltpu.VMEM((tok, LANES), F32),
            pltpu.VMEM((tok, LANES), BF16),
            pltpu.VMEM((tok, LANES), BF16),
            pltpu.VMEM((chunks, LANES, LANES), F32),
            pltpu.VMEM((chunks, LANES, LANES), F32),
            pltpu.VMEM((2, chunks, 1, LANES), F32),
            pltpu.VMEM((z_count, 2, rows_s + 8, LANES), BF16),
            pltpu.VMEM((ep_count, rows_s + 8, LANES), BF16),
            pltpu.VMEM((ep_count, rows_s, LANES), BF16),
            pltpu.VMEM((ep_count, rows_s, LANES), BF16),
            pltpu.VMEM((2, 4, 2, tok // 4, LANES), BF16),
            pltpu.VMEM((2, 4, 2, tok // 4, LANES), BF16),
            pltpu.VMEM((2, 4, 2, tok // 4, LANES), BF16),
            dma((19,)),
            dma((9,)),
            dma((9,)),
            dma((2, 2, 20)),
            dma((2, 2, 20)),
            dma((2, 2, 2, 4)),
            dma((2, 2, 2, 4)),
            dma((2, 2, 20)),
            dma((2, 2, 20)),
        ],
        compiler_params=pltpu.CompilerParams(collective_id=0, has_side_effects=True),
    )(
        q,
        right,
        left,
        v,
        bounds,
        spikes,
        gain.reshape(1, -1),
        emit,
        rows,
        rows_gain.reshape(1, -1),
        ids.T,
        shares.T,
        switch.transpose(0, 2, 1),
        widen.transpose(0, 2, 1),
        shrink,
    )


def solution(mesh):
    ep, tp = mesh.shape["ep"], mesh.shape["tp"]
    split = Mesh(mesh.devices.reshape(ep // 2, 2, tp // 4, 4), ("z", "c", "y", "x"))
    e, f = ("z", "c"), ("y", "x")
    return jax.shard_map(
        per_device,
        mesh=split,
        in_specs=(
            P(e, f),
            P(e, f),
            P(e, f),
            P(e, f),
            P(None, f),
            P(f, e),
            P(f),
            P(f, None),
            P(e, None),
            P(),
            P(e, None),
            P(e, None),
            P(e, None, f),
            P(e, None, f),
            P(e, f, None),
        ),
        out_specs=(P(e, f), P(e, f)),
        check_vma=False,
    )
```
